512 devices in a mesh: ep: 128 (over z, x, core), tp: 4 (over y).
Axes of the slice: x: 4, y: 4, z: 16, core: 2. Of those that a mesh axis runs over, the one named last changes fastest.
Arguments:
- tokens: bfloat16 [2048, 1024], P('ep'), may hold values from -6 to 6
- memory: float32 [2048, 4, 128, 256], P('ep', 'tp'), may hold values from -6 to 6
- log_scale: float32 [2048, 4], P('ep', 'tp'), may hold values from -1 to 130
- mix_gain_in: float32 [1024], replicated, may hold values from 0.1 to 1.9
- w_query: bfloat16 [1024, 512], P(None, 'tp'), may hold values from -0.1875 to 0.1875
- w_key: bfloat16 [1024, 512], P(None, 'tp'), may hold values from -0.1875 to 0.1875
- w_value: bfloat16 [1024, 1024], P(None, 'tp'), may hold values from -0.1875 to 0.1875
- w_igate: bfloat16 [1024, 4], P(None, 'tp'), may hold values from -0.1875 to 0.1875
- w_fgate: bfloat16 [1024, 4], P(None, 'tp'), may hold values from -0.1875 to 0.1875
- igate_bias: float32 [4], P('tp'), may hold values from -1 to 1
- fgate_bias: float32 [4], P('tp'), may hold values from 0 to 4
- head_gain: float32 [1024], P('tp'), may hold values from 0.1 to 1.9
- w_output: bfloat16 [1024, 1024], P('tp'), may hold values from -0.1875 to 0.1875
- mix_gain_out: float32 [1024], replicated, may hold values from 0.1 to 1.9
- ffn_gain_in: float32 [1024], replicated, may hold values from 0.1 to 1.9
- routes: int32 [2048, 6], P('ep'), may hold values from 0 to 127, all different within a row; in each aligned block of 16 rows (0 to 15, 16 to 31, ...) at most 2 rows name the same one
- route_weights: float32 [2048, 6], P('ep'), may hold values from 0.1 to 1
- expert_gate: bfloat16 [128, 1024, 1024], P('ep', None, 'tp'), may hold values from -0.1875 to 0.1875
- expert_up: bfloat16 [128, 1024, 1024], P('ep', None, 'tp'), may hold values from -0.1875 to 0.1875
- expert_down: bfloat16 [128, 1024, 1024], P('ep', 'tp'), may hold values from -0.9375 to 0.9375
- ffn_gain_out: float32 [1024], P('tp'), may hold values from 0.1 to 1.9
Outputs:
- output: bfloat16 [2048, 1024], P('ep', 'tp')
The draws below stay inside these ranges and needn't reach their ends.
Inputs may be any that keep to these rules, and one draw needn't show every extreme that they name: `routes`: among the 16 tokens of one index of ep no expert is named by more than 2 tokens, and in every draw some expert is named by exactly 2 of them.
All inputs are finite; a program needn't handle non-finite values.
Results may differ from the reference program's by a relative error of at most 0.02.
Values may be sent and summed in bfloat16 or wider, within the bound.
A program may use at most 64 MiB of HBM per device.

```python
import math
import jax
import jax.numpy as jnp
import numpy as np
from jax import lax

D = 1024
HEADS = 4
KEY_DIM = 128
VALUE_DIM = 256
EXPERT_WIDTH = 1024
TOP_K = 6
SEQ_G = 16
EXPERTS = 128
CAP = 2
BATCH = 2048
N_EP = 128


def draw_log_scale(key, part):
    base_key = jax.random.fold_in(key, 11)
    values = jax.random.uniform(base_key, (BATCH, HEADS), jnp.float32, -1.0, 3.0)
    return values


def draw_expert_down(key, part):
    noise_key = jax.random.fold_in(key, 21)
    column_key = jax.random.fold_in(key, 22)
    raw = jnp.clip(jax.random.normal(noise_key, (EXPERTS, EXPERT_WIDTH, D), jnp.float32), -4.0, 4.0)
    spot = (jnp.arange(D, dtype=jnp.float32) + 0.5) / D
    jitter = jax.random.uniform(column_key, (D,), jnp.float32, -0.4, 0.4)
    ramp = 1.2 * (2.0 * spot - 1.0)
    scale = jnp.exp(ramp + jitter) * EXPERT_WIDTH ** (-0.5)
    return (raw * scale[None, None, :]).astype(jnp.bfloat16)


def block_scale(stream_key, dims, pieces, smallest, largest):
    loudness, own = 1.0, jax.random.fold_in(stream_key, 6)
    for dim, parts in pieces:
        heights = jnp.exp(jax.random.uniform(jax.random.fold_in(own, dim), (parts,), jnp.float32, smallest / len(pieces), largest / len(pieces)))
        loudness = loudness * jnp.repeat(heights, dims[dim] // parts).reshape([-1 if axis == dim else 1 for axis in range(len(dims))])
    return loudness


def assign_block(rng, own, number, rows, number_of, top, reach, lean):
    ranking = jax.random.permutation(rng, number_of)
    crowded, usual = portions_of(number_of, rows * top, reach, lean, True), portions_of(number_of, rows * top, reach, lean, False)
    places = jnp.arange(number_of)

    def named(sizes, turn):
        used = int((sizes > 0).sum())
        fixed = max(1, used // 4)
        moved = fixed + (places - fixed + turn * (used - fixed)) % max(1, number_of - fixed)
        return jnp.zeros((number_of,), jnp.int32).at[ranking[jnp.where(places < fixed, places, moved)]].set(jnp.asarray(sizes, jnp.int32))

    sizes = jnp.where(number % 4 == 0, named(crowded, number // 4), named(usual, number - number // 4 - 1))
    mixed = jax.random.permutation(jax.random.fold_in(own, 3), number_of)
    giver, taker = mixed[0:number_of // 2 * 2:2], mixed[1:number_of // 2 * 2:2]
    slack = jnp.minimum(sizes[giver] - 1, reach - sizes[taker]) // 2
    slack = jnp.where((giver == ranking[0]) | (taker == ranking[0]) | (sizes[taker] == 0), 0, jnp.maximum(slack, 0))
    moved = jax.random.randint(jax.random.fold_in(own, 4), (number_of // 2,), 0, 1 << 20) % (slack + 1)
    sizes = sizes.at[giver].add(-moved).at[taker].add(moved)
    members = jnp.searchsorted(jnp.cumsum(sizes), jnp.arange(rows * top), side="right").astype(jnp.int32)
    listing = members.reshape(top, rows).T
    listing = listing[jax.random.permutation(jax.random.fold_in(own, 1), rows)]
    turn = jax.random.randint(jax.random.fold_in(own, 2), (rows, 1), 0, top)
    return jnp.take_along_axis(listing, (jnp.arange(top)[None, :] + turn) % top, axis=1)


def portions_of(number_of, total, reach, lean, full):
    portions = [(1 << 20) // math.isqrt(rank ** lean) + 1 for rank in range(1, number_of + 1)]
    largest = reach if full else min(reach, max(-(-total // number_of), total * portions[0] // sum(portions)))
    least = 1 if total - largest >= number_of - 1 else 0
    counts, rest = [largest] + [least] * (number_of - 1), total - largest - least * (number_of - 1)
    while rest > 0:
        candidates = [i for i in range(1, number_of) if counts[i] < largest] or [i for i in range(1, number_of) if counts[i] < reach]
        pool, remaining = sum([portions[i] for i in candidates]), rest
        for i in candidates:
            addition = min(reach - counts[i], max(1, remaining * portions[i] // pool), rest)
            counts[i] = counts[i] + addition
            rest = rest - addition
    return np.array(counts)


def noise(key, shape, scale, bound, split=(), held_as=jnp.bfloat16):
    values = jax.random.normal(key, shape, jnp.float32) * scale
    if len(split) > 0:
        values = block_scale(key, shape, split, -0.22, 0.18) * values
    return jnp.clip(values, min=-bound, max=bound).astype(held_as)


def setup_inputs(seed: int = 0) -> dict:
    splits = jax.random.split(jax.random.key(seed), 22)
    tokens = noise(splits[0], (BATCH, D), 1.0, 6.0, ((0, 128),))
    memory = noise(splits[1], (BATCH, HEADS, KEY_DIM, VALUE_DIM), 1.0, 6.0, ((0, 128), (1, 4)), jnp.float32)
    log_scale = draw_log_scale(jax.random.fold_in(splits[21], 71), 0)
    mix_gain_in = jnp.clip(1.0 + 0.18 * jax.random.normal(splits[3], (D,), jnp.float32), 0.1, 1.9)
    w_query = noise(splits[4], (D, HEADS * KEY_DIM), D ** -0.5, 0.1875, ((1, 4),))
    w_key = noise(splits[5], (D, HEADS * KEY_DIM), D ** -0.5, 0.1875, ((1, 4),))
    w_value = noise(splits[6], (D, HEADS * VALUE_DIM), D ** -0.5, 0.1875, ((1, 4),))
    w_igate = noise(splits[7], (D, HEADS), D ** -0.5, 0.1875, ((1, 4),))
    w_fgate = noise(splits[8], (D, HEADS), D ** -0.5, 0.1875, ((1, 4),))
    igate_bias = jnp.clip(jax.random.uniform(splits[9], (HEADS,), jnp.float32, -1.0, 1.0) * block_scale(splits[9], (HEADS,), ((0, 4),), -0.4, 0.0), -1.0, 1.0)
    fgate_bias = jnp.clip(4.0 * jax.random.uniform(splits[10], (HEADS,), jnp.float32) ** block_scale(splits[10], (HEADS,), ((0, 4),), -0.2, 0.2), 0.0, 4.0)
    head_gain = jnp.clip(1.0 + 0.18 * jax.random.normal(splits[11], (HEADS * VALUE_DIM,), jnp.float32), 0.1, 1.9)
    w_output = noise(splits[12], (HEADS * VALUE_DIM, D), (HEADS * VALUE_DIM) ** -0.5, 0.1875, ((0, 4),))
    mix_gain_out = jnp.clip(1.0 + 0.18 * jax.random.normal(splits[13], (D,), jnp.float32), 0.1, 1.9)
    ffn_gain_in = jnp.clip(1.0 + 0.18 * jax.random.normal(splits[14], (D,), jnp.float32), 0.1, 1.9)
    routes_keys = jax.random.split(jax.random.fold_in(splits[15], 1), BATCH // SEQ_G)
    routes_turns = jax.random.permutation(jax.random.fold_in(splits[15], 3), BATCH // SEQ_G)
    routes = jax.vmap(lambda own, number: assign_block(jax.random.fold_in(splits[15], 2), own, number, SEQ_G, EXPERTS, TOP_K, CAP, 1))(routes_keys, routes_turns).reshape((BATCH, TOP_K))
    route_weights = jnp.clip(jnp.exp(math.log(1.0) - 2.3025851 * jax.random.uniform(splits[16], (BATCH, TOP_K), jnp.float32) ** block_scale(splits[16], (BATCH, TOP_K), ((0, 128),), -0.2, 0.2)), 0.1, 1.0)
    expert_gate = noise(splits[17], (EXPERTS, D, EXPERT_WIDTH), D ** -0.5, 0.1875, ((0, 128), (2, 4)))
    expert_up = noise(splits[18], (EXPERTS, D, EXPERT_WIDTH), D ** -0.5, 0.1875, ((0, 128), (2, 4)))
    expert_down = draw_expert_down(jax.random.fold_in(splits[21], 71), 0)
    ffn_gain_out = jnp.clip(1.0 + 0.18 * jax.random.normal(splits[20], (D,), jnp.float32), 0.1, 1.9)
    return dict(tokens=tokens, memory=memory, log_scale=log_scale, mix_gain_in=mix_gain_in, w_query=w_query, w_key=w_key, w_value=w_value, w_igate=w_igate, w_fgate=w_fgate, igate_bias=igate_bias, fgate_bias=fgate_bias, head_gain=head_gain, w_output=w_output, mix_gain_out=mix_gain_out, ffn_gain_in=ffn_gain_in, routes=routes, route_weights=route_weights, expert_gate=expert_gate, expert_up=expert_up, expert_down=expert_down, ffn_gain_out=ffn_gain_out)


EPS = 1e-06

def rms_scale(values):
    return lax.rsqrt(lax.optimization_barrier(jnp.mean(values * values, axis=-1, keepdims=True)) + EPS)

def reference(tokens, memory, log_scale, mix_gain_in, w_query, w_key, w_value, w_igate, w_fgate, igate_bias, fgate_bias, head_gain, w_output, mix_gain_out, ffn_gain_in, routes, route_weights, expert_gate, expert_up, expert_down, ffn_gain_out):
    f32 = jnp.float32
    bf16 = jnp.bfloat16
    xf = tokens.astype(f32)
    normed = (xf * rms_scale(xf) * mix_gain_in).astype(bf16)
    query = jnp.dot(normed, w_query, preferred_element_type=f32).reshape(BATCH, HEADS, KEY_DIM) * KEY_DIM ** (-0.5)
    keys = jnp.dot(normed, w_key, preferred_element_type=f32).reshape(BATCH, HEADS, KEY_DIM)
    values = jnp.dot(normed, w_value, preferred_element_type=f32).reshape(BATCH, HEADS, VALUE_DIM)
    in_pre = jnp.dot(normed, w_igate, preferred_element_type=f32) + igate_bias
    forget_log = jax.nn.log_sigmoid(jnp.dot(normed, w_fgate, preferred_element_type=f32) + fgate_bias)
    carried = forget_log + log_scale
    new_max = jnp.maximum(carried, in_pre)
    carry_weight = jnp.exp(carried - new_max)
    fresh_weight = jnp.exp(in_pre - new_max)
    recall = jnp.einsum('bhk,bhkv->bhv', query, memory, precision=lax.Precision.HIGHEST)
    match = lax.optimization_barrier(jnp.sum(query * keys, axis=-1))
    read = carry_weight[..., None] * recall + (fresh_weight * match)[..., None] * values
    headout = (read * rms_scale(read) * head_gain.reshape(HEADS, VALUE_DIM)).astype(bf16)
    per_head = jnp.einsum('bhv,hvd->bhd', headout.astype(f32), w_output.reshape(HEADS, VALUE_DIM, D).astype(f32)).astype(bf16)
    mixed = lax.optimization_barrier(jnp.sum(per_head.astype(f32), axis=1))
    resid = (xf + mixed * rms_scale(mixed) * mix_gain_out).astype(bf16)
    rf = resid.astype(f32)
    ffn_in = (rf * rms_scale(rf) * ffn_gain_in).astype(bf16)
    rows_total = BATCH * TOP_K
    limit = N_EP * CAP
    flat = routes.reshape(-1).astype(jnp.int32)

    def per_expert(done, expert):
        found = jnp.nonzero(flat == expert, size=limit, fill_value=rows_total)[0].astype(jnp.int32)
        token = jnp.minimum(found // TOP_K, BATCH - 1)
        picked = jnp.take(ffn_in, token, axis=0)
        gate = jnp.dot(picked, expert_gate[expert], preferred_element_type=f32)
        up = jnp.dot(picked, expert_up[expert], preferred_element_type=f32)
        act = (jax.nn.silu(gate) * up).astype(bf16)
        blocks = jnp.einsum('rtf,tfd->rtd', act.reshape(limit, HEADS, EXPERT_WIDTH // HEADS).astype(f32), expert_down[expert].reshape(HEADS, EXPERT_WIDTH // HEADS, D).astype(f32)).astype(bf16)
        result = lax.optimization_barrier(jnp.sum(blocks.astype(f32), axis=1)).astype(bf16)
        done = done.at[found].set(result, mode='drop')
        return (done, None)
    done, _ = lax.scan(per_expert, jnp.zeros((rows_total, D), bf16), jnp.arange(EXPERTS, dtype=jnp.int32))
    expert_rows = done.reshape(BATCH, TOP_K, D).astype(f32)
    routed = lax.optimization_barrier(jnp.sum(route_weights[..., None] * expert_rows, axis=1))
    return (rf + routed * rms_scale(routed) * ffn_gain_out).astype(bf16)
```

```python
import functools

import jax
import jax.numpy as jnp
from jax import lax
from jax.experimental import pallas as pl
from jax.experimental.pallas import tpu as pltpu
from jax.sharding import PartitionSpec as P

EPS = 1e-06
MESH = pl.DeviceIdType.MESH
LANES = 128
NX = 4
NY = 4
CHUNKS = 4


def offset_of(rank):
    return (rank + 1) // 2 if rank % 2 else -(rank // 2)


def rms(values):
    return lax.rsqrt(jnp.mean(values * values, axis=-1, keepdims=True) + EPS)


def kernel(
    nz,
    tokens_h, memory_h, scale_h, gain_in_h, wq_h, wk_h, wv_h, wi_h, wf_h, bi_h, bf_h,
    head_gain_h, wo_h, gain_out_h, gain_ffn_h, routes_h, weights_h, eg_h, eu_h, ed_h, gain_last_h,
    out_ref,
    tokens_v, memory_v, scale_v, gain_in_v, wq_v, wk_v, wv_v, wi_v, wf_v, bi_v, bf_v,
    head_gain_v, wo_v, gain_out_v, gain_ffn_v, routes_v, weights_v, eg_v, eu_v, ed_v, gain_last_v,
    recall_v, mix_v, pick_v, pull_hi_v, pull_lo_v, msg_v, rows_v, part_v, red_v, back_v, home_v, last_v, resid_v, total_v,
    load_sem, mix_send, mix_recv, out_send, self_send, in_recv, self_recv, gat_send, gat_recv,
    red_send, red_recv, ret_send, ret_self_send, ret_recv, ret_self_recv, last_send, last_recv,
):
    f32, bf16 = jnp.float32, jnp.bfloat16
    seqs, width = tokens_v.shape
    pieces = width // LANES
    slots = 2 * nz
    per = slots // CHUNKS
    experts = nz * NX * 2

    me = lax.axis_index("ep")
    y = lax.axis_index("tp")
    c = me % 2
    x = (me // 2) % NX
    z = me // (2 * NX)
    px = (y + NX - x) % NX
    mine = px == x

    def target(slot, sign):
        zz = (z + nz + sign * offset_of(slot // 2)) % nz
        cc = c if slot % 2 == 0 else 1 - c
        return (zz * NX + px) * 2 + cc

    def peer(step):
        return (y + step) % NY

    pairs = [
        (routes_h, routes_v), (weights_h, weights_v), (tokens_h, tokens_v), (gain_in_h, gain_in_v),
        (wq_h, wq_v), (wk_h, wk_v), (wv_h, wv_v), (wi_h, wi_v), (wf_h, wf_v), (bi_h, bi_v), (bf_h, bf_v),
        (scale_h, scale_v), (memory_h, memory_v), (head_gain_h, head_gain_v), (wo_h, wo_v),
        (gain_out_h, gain_out_v), (gain_ffn_h, gain_ffn_v), (eg_h, eg_v), (eu_h, eu_v), (ed_h, ed_v),
        (gain_last_h, gain_last_v),
    ]
    loads = {}
    for i, (src, dst) in enumerate(pairs):
        loads[id(dst)] = pltpu.make_async_copy(src, dst, load_sem.at[i])
        loads[id(dst)].start()

    def ready(*refs):
        for ref in refs:
            loads[id(ref)].wait()

    barrier = pltpu.get_barrier_semaphore()
    for step in range(1, NY):
        pl.semaphore_signal(barrier, inc=1, device_id=(me, peer(step)), device_id_type=MESH)
    for slot in range(1, slots):
        pl.semaphore_signal(barrier, inc=1, device_id=(target(slot, 1), y), device_id_type=MESH)

    @pl.when(jnp.logical_not(mine))
    def _():
        pl.semaphore_signal(barrier, inc=1, device_id=(target(0, 1), y), device_id_type=MESH)

    ready(routes_v, weights_v)
    expert_row = lax.broadcasted_iota(jnp.int32, (experts, LANES), 0)
    named = jnp.zeros((experts, LANES), f32)
    weight = jnp.zeros((experts, LANES), f32)
    for j in range(routes_v.shape[0]):
        hit = expert_row == routes_v[j : j + 1, :]
        named = jnp.where(hit, 1.0, named)
        weight = jnp.where(hit, weights_v[j : j + 1, :], weight)
    row = lax.broadcasted_iota(jnp.int32, (LANES, LANES), 0)
    col = lax.broadcasted_iota(jnp.int32, (LANES, LANES), 1)
    before = jnp.where((row // seqs == col // seqs) & (row < col), 1.0, 0.0).astype(bf16)
    count = jnp.dot(named.astype(bf16), before, preferred_element_type=f32)
    first = jnp.where(count < 0.5, named, 0.0)
    second = named - first
    hi = weight.astype(bf16).astype(f32)
    lo = weight - hi
    sel = jnp.concatenate([first, second], axis=0).astype(bf16)
    sel_hi = jnp.concatenate([first * hi, second * hi], axis=0).astype(bf16)
    sel_lo = jnp.concatenate([first * lo, second * lo], axis=0).astype(bf16)
    lines = slots * 2 * pieces
    r2 = lax.broadcasted_iota(jnp.int32, (lines, 2 * experts), 0)
    c2 = lax.broadcasted_iota(jnp.int32, (lines, 2 * experts), 1)
    rank = r2 // (4 * pieces)
    dz = jnp.where(rank % 2 == 1, (rank + 1) // 2, -(rank // 2))
    dc = (r2 // (2 * pieces)) % 2
    goal = (((z + nz + dz) % nz) * NX + px) * 2 + jnp.where(dc == 0, c, 1 - c)
    choose = jnp.where(c2 == goal + ((r2 // pieces) % 2) * experts, 1.0, 0.0).astype(bf16)
    r3 = lax.broadcasted_iota(jnp.int32, (lines, LANES), 0)
    c3 = lax.broadcasted_iota(jnp.int32, (lines, LANES), 1)
    same = (r3 % pieces) == (c3 // seqs)

    def spread(matrix):
        return jnp.where(same, jnp.dot(choose, matrix, preferred_element_type=f32), 0.0)

    pick_v[...] = spread(sel).astype(bf16)
    pull_hi_v[...] = spread(sel_hi).T.astype(bf16)
    pull_lo_v[...] = spread(sel_lo).T.astype(bf16)

    half = 2 * per
    order = jnp.where((row // half == col % pieces) & (row % half == col // pieces), 1.0, 0.0).astype(bf16)
    disorder = jnp.where((col // half == row % pieces) & (col % half == row // pieces), 1.0, 0.0).astype(bf16)

    ready(tokens_v, gain_in_v)
    xf = tokens_v[...].astype(f32)
    normed = (xf * rms(xf) * gain_in_v[...]).astype(bf16)
    ready(wq_v, wk_v, wv_v)
    key_dim = wq_v.shape[1]
    query = jnp.dot(normed, wq_v[...], preferred_element_type=f32) * key_dim ** (-0.5)
    keys = jnp.dot(normed, wk_v[...], preferred_element_type=f32)
    values = jnp.dot(normed, wv_v[...], preferred_element_type=f32)
    ready(wi_v, wf_v, bi_v, bf_v, scale_v)
    nf = normed.astype(f32)
    in_pre = jnp.sum(nf * wi_v[...].astype(f32), axis=-1, keepdims=True) + bi_v[...]
    fg = jnp.sum(nf * wf_v[...].astype(f32), axis=-1, keepdims=True) + bf_v[...]
    forget_log = jnp.minimum(fg, 0.0) - jnp.log1p(jnp.exp(-jnp.abs(fg)))
    tr = lax.broadcasted_iota(jnp.int32, (seqs, seqs), 0)
    tc = lax.broadcasted_iota(jnp.int32, (seqs, seqs), 1)
    log_scale = jnp.sum(
        jnp.where(tr == tc, jnp.broadcast_to(scale_v[...], (seqs, seqs)), 0.0), axis=-1, keepdims=True
    )
    carried = forget_log + log_scale
    new_max = jnp.maximum(carried, in_pre)
    carry_weight = jnp.exp(carried - new_max)
    fresh_weight = jnp.exp(in_pre - new_max)
    match = jnp.sum(query * keys, axis=-1, keepdims=True)
    turned = query.T
    ready(memory_v)
    for s in range(seqs):
        recall_v[s : s + 1, :] = jnp.sum(turned[:, s : s + 1] * memory_v[s], axis=0, keepdims=True)
    read = carry_weight * recall_v[...] + (fresh_weight * match) * values
    ready(head_gain_v, wo_v)
    headout = (read * rms(read) * head_gain_v[...]).astype(bf16)
    mix_v[y] = jnp.dot(headout, wo_v[...], preferred_element_type=f32).astype(bf16)

    pl.semaphore_wait(barrier, NY - 1 + slots - jnp.where(mine, 1, 0))

    def to_peers(ref, send_sem, recv_sem):
        copies = []
        for step in range(1, NY):
            copy = pltpu.make_async_remote_copy(
                src_ref=ref.at[y], dst_ref=ref.at[y], send_sem=send_sem.at[step], recv_sem=recv_sem.at[step],
                device_id=(me, peer(step)), device_id_type=MESH,
            )
            copy.start()
            copies.append(copy)
        for step in range(1, NY):
            source = peer(NY - step)
            pltpu.make_async_remote_copy(
                src_ref=ref.at[source], dst_ref=ref.at[source], send_sem=send_sem.at[step],
                recv_sem=recv_sem.at[step], device_id=(me, peer(step)), device_id_type=MESH,
            ).wait_recv()
        return copies

    mix_copies = to_peers(mix_v, mix_send, mix_recv)
    mixed = mix_v[0].astype(f32)
    for i in range(1, NY):
        mixed = mixed + mix_v[i].astype(f32)
    ready(gain_out_v, gain_ffn_v)
    resid = (xf + mixed * rms(mixed) * gain_out_v[...]).astype(bf16)
    rf = resid.astype(f32)
    resid_v[...] = rf
    ffn_in = (rf * rms(rf) * gain_ffn_v[...]).astype(bf16)

    def stacked(array):
        return jnp.concatenate([array[:, k * LANES : (k + 1) * LANES] for k in range(pieces)], axis=0)

    message = jnp.dot(pick_v[...], stacked(ffn_in), preferred_element_type=f32).astype(bf16)
    msg_v[...] = message.reshape(slots, 2 * pieces, LANES)

    def away(slot, src, dst, sign, send_sem, recv_sem):
        return pltpu.make_async_remote_copy(
            src_ref=src, dst_ref=dst, send_sem=send_sem, recv_sem=recv_sem,
            device_id=(target(slot, sign), y), device_id_type=MESH,
        )

    own = away(0, msg_v.at[0], rows_v.at[y, 0], 1, self_send, self_recv)

    @pl.when(jnp.logical_not(mine))
    def _():
        own.start()

    @pl.when(mine)
    def _():
        rows_v[y, 0] = msg_v[0]

    for slot in range(1, slots):
        away(slot, msg_v.at[slot], rows_v.at[y, slot], 1, out_send, in_recv.at[slot // per]).start()

    ready(eg_v, eu_v, ed_v)

    def arrive(g):
        lo_slot = 1 if g == 0 else g * per
        region = rows_v.at[y, pl.ds(lo_slot, (g + 1) * per - lo_slot)]
        away(0, region, region, 1, out_send, in_recv.at[g]).wait_recv()
        if g == 0:

            @pl.when(jnp.logical_not(mine))
            def _():
                own.wait_recv()

        for step in range(1, NY):
            piece = rows_v.at[y, pl.ds(g * per, per)]
            pltpu.make_async_remote_copy(
                src_ref=piece, dst_ref=piece, send_sem=gat_send, recv_sem=gat_recv.at[step, g],
                device_id=(me, peer(step)), device_id_type=MESH,
            ).start()

    def expert(g):
        for step in range(1, NY):
            source = peer(NY - step)
            piece = rows_v.at[source, pl.ds(g * per, per)]
            pltpu.make_async_remote_copy(
                src_ref=piece, dst_ref=piece, send_sem=gat_send, recv_sem=gat_recv.at[step, g],
                device_id=(me, peer(step)), device_id_type=MESH,
            ).wait_recv()
        side = jnp.concatenate(
            [rows_v[i, g * per : (g + 1) * per].reshape(per * 2 * pieces, LANES) for i in range(NY)], axis=1
        )
        sorted_rows = jnp.dot(order, side, preferred_element_type=f32).astype(bf16)
        inputs = jnp.concatenate(
            [
                jnp.concatenate(
                    [sorted_rows[k * half : (k + 1) * half, i * LANES : (i + 1) * LANES] for k in range(pieces)],
                    axis=1,
                )
                for i in range(NY)
            ],
            axis=0,
        )
        gate = jnp.dot(inputs, eg_v[...], preferred_element_type=f32)
        up = jnp.dot(inputs, eu_v[...], preferred_element_type=f32)
        act = (jax.nn.silu(gate) * up).astype(bf16)
        part = jnp.dot(act, ed_v[...], preferred_element_type=f32).astype(bf16)
        for i in range(NY):
            part_v[g, i] = part[i * half : (i + 1) * half, :]
        for step in range(1, NY):
            pltpu.make_async_remote_copy(
                src_ref=part_v.at[g, peer(step)], dst_ref=red_v.at[g, step], send_sem=red_send,
                recv_sem=red_recv.at[step, g], device_id=(me, peer(step)), device_id_type=MESH,
            ).start()

    back_own = away(0, back_v.at[0], home_v.at[0], -1, ret_self_send, ret_self_recv)

    def give_back(g):
        total = part_v[g, y].astype(f32)
        for step in range(1, NY):
            pltpu.make_async_remote_copy(
                src_ref=part_v.at[g, peer(step)], dst_ref=red_v.at[g, step], send_sem=red_send,
                recv_sem=red_recv.at[step, g], device_id=(me, peer(step)), device_id_type=MESH,
            ).wait_recv()
        for step in range(1, NY):
            total = total + red_v[g, step].astype(f32)
        lined = jnp.dot(disorder, stacked(total.astype(bf16)), preferred_element_type=f32).astype(bf16)
        back_v[g * per : (g + 1) * per] = lined.reshape(per, 2 * pieces, LANES)
        for slot in range(g * per, (g + 1) * per):
            if slot == 0:

                @pl.when(jnp.logical_not(mine))
                def _():
                    back_own.start()

                @pl.when(mine)
                def _():
                    home_v[0] = back_v[0]

            else:
                away(slot, back_v.at[slot], home_v.at[slot], -1, ret_send, ret_recv.at[g]).start()

    for step in range(CHUNKS + 2):
        if step < CHUNKS:
            arrive(step)
        if 1 <= step <= CHUNKS:
            expert(step - 1)
        if step >= 2:
            give_back(step - 2)

    routed = jnp.zeros((LANES, LANES), f32)
    for g in range(CHUNKS):
        lo_slot = 1 if g == 0 else g * per
        region = home_v.at[pl.ds(lo_slot, (g + 1) * per - lo_slot)]
        away(0, region, region, -1, ret_send, ret_recv.at[g]).wait_recv()
        if g == 0:

            @pl.when(jnp.logical_not(mine))
            def _():
                back_own.wait_recv()

        block = home_v[g * per : (g + 1) * per].reshape(per * 2 * pieces, LANES)
        span = slice(g * per * 2 * pieces, (g + 1) * per * 2 * pieces)
        routed = routed + jnp.dot(pull_hi_v[:, span], block, preferred_element_type=f32)
        routed = routed + jnp.dot(pull_lo_v[:, span], block, preferred_element_type=f32)
    flat = jnp.concatenate([routed[k * seqs : (k + 1) * seqs, :] for k in range(pieces)], axis=1)
    last_v[y] = flat.astype(bf16)
    last_copies = to_peers(last_v, last_send, last_recv)
    total = last_v[0].astype(f32)
    for i in range(1, NY):
        total = total + last_v[i].astype(f32)
    total_v[...] = total * rms(total)
    ready(gain_last_v)
    quarter = width // NY
    mark = pl.ds(pl.multiple_of(y * quarter, quarter), quarter)
    out_ref[...] = (resid_v[:, mark] + total_v[:, mark] * gain_last_v[...]).astype(bf16)

    for copy in mix_copies + last_copies:
        copy.wait_send()
    rest = msg_v.at[pl.ds(1, slots - 1)]
    away(0, rest, rest, 1, out_send, self_recv).wait_send()
    rest = back_v.at[pl.ds(1, slots - 1)]
    away(0, rest, rest, 1, ret_send, self_recv).wait_send()

    @pl.when(jnp.logical_not(mine))
    def _():
        own.wait_send()
        back_own.wait_send()

    everything = rows_v.at[pl.ds(0, NY - 1)]
    away(0, everything, everything, 1, gat_send, self_recv).wait_send()
    everything = red_v.at[:, pl.ds(1, NY - 1)]
    away(0, everything, everything, 1, red_send, self_recv).wait_send()


def per_device(
    nz, tokens, memory, log_scale, mix_gain_in, w_query, w_key, w_value, w_igate, w_fgate, igate_bias, fgate_bias,
    head_gain, w_output, mix_gain_out, ffn_gain_in, routes, route_weights, expert_gate, expert_up, expert_down,
    ffn_gain_out,
):
    f32, bf16 = jnp.float32, jnp.bfloat16
    seqs, width = tokens.shape
    pieces = width // LANES
    key_dim, value_dim = memory.shape[2:]
    slots = 2 * nz
    per = slots // CHUNKS
    lines = slots * 2 * pieces
    hidden = expert_gate.shape[2]
    operands = [
        tokens, memory[:, 0], log_scale.T, mix_gain_in[None], w_query, w_key, w_value, w_igate.T, w_fgate.T,
        igate_bias[None], fgate_bias[None], head_gain[None], w_output, mix_gain_out[None], ffn_gain_in[None],
        jnp.tile(routes.T, (1, LANES // seqs)), jnp.tile(route_weights.T, (1, LANES // seqs)),
        expert_gate[0], expert_up[0], expert_down[0], ffn_gain_out[None],
    ]
    dma, vmem = pltpu.SemaphoreType.DMA, pltpu.VMEM
    scratch = [vmem(a.shape, a.dtype) for a in operands] + [
        vmem((seqs, value_dim), f32),
        vmem((NY, seqs, width), bf16),
        vmem((lines, LANES), bf16),
        vmem((LANES, lines), bf16),
        vmem((LANES, lines), bf16),
        vmem((slots, 2 * pieces, LANES), bf16),
        vmem((NY, slots, 2 * pieces, LANES), bf16),
        vmem((CHUNKS, NY, 2 * per, width), bf16),
        vmem((CHUNKS, NY, 2 * per, width), bf16),
        vmem((slots, 2 * pieces, LANES), bf16),
        vmem((slots, 2 * pieces, LANES), bf16),
        vmem((NY, seqs, width), bf16),
        vmem((seqs, width), f32),
        vmem((seqs, width), f32),
        dma((len(operands),)), dma((NY,)), dma((NY,)), dma, dma, dma((CHUNKS,)), dma, dma, dma((NY, CHUNKS)),
        dma, dma((NY, CHUNKS)), dma, dma, dma((CHUNKS,)), dma, dma((NY,)), dma((NY,)),
    ]
    return pl.pallas_call(
        functools.partial(kernel, nz),
        out_shape=jax.ShapeDtypeStruct((seqs, width // NY), bf16),
        in_specs=[pl.BlockSpec(memory_space=pltpu.HBM)] * len(operands),
        out_specs=pl.BlockSpec(memory_space=pltpu.VMEM),
        scratch_shapes=scratch,
        compiler_params=pltpu.CompilerParams(collective_id=0, has_side_effects=True, vmem_limit_bytes=32 << 20),
    )(*operands)


def solution(mesh):
    nz = mesh.shape["ep"] // (2 * NX)
    return jax.shard_map(
        functools.partial(per_device, nz),
        mesh=mesh,
        in_specs=(
            P("ep", None), P("ep", "tp", None, None), P("ep", "tp"), P(), P(None, "tp"), P(None, "tp"),
            P(None, "tp"), P(None, "tp"), P(None, "tp"), P("tp"), P("tp"), P("tp"), P("tp", None), P(), P(),
            P("ep", None), P("ep", None), P("ep", None, "tp"), P("ep", None, "tp"), P("ep", "tp", None), P("tp"),
        ),
        out_specs=P("ep", "tp"),
        check_vma=False,
    )
```

```python
import functools

import jax
import jax.numpy as jnp
from jax import lax
from jax.experimental import pallas as pl
from jax.experimental.pallas import tpu as pltpu
from jax.sharding import PartitionSpec as P

EPS = 1e-06
MESH = pl.DeviceIdType.MESH
LANES = 128
NX = 4
NY = 4
CHUNKS = 4
ORDER = (0, 1, 3, 2)


def rms(values):
    return lax.rsqrt(jnp.mean(values * values, axis=-1, keepdims=True) + EPS)


def kernel(
    nz,
    tokens_h, memory_h, scale_h, gain_in_h, wq_h, wk_h, wv_h, wi_h, wf_h, bi_s, bf_s,
    head_gain_h, wo_h, gain_out_h, gain_ffn_h, routes_h, weights_h, eg_h, eu_h, ed_h, gain_last_h,
    out_ref,
    tokens_v, memory_v, scale_v, gain_in_v, wq_v, wk_v, wv_v, wi_v, wf_v,
    head_gain_v, wo_v, gain_out_v, gain_ffn_v, routes_v, weights_v, eg_v, eu_v, ed_v, gain_last_v,
    recall_v, mix_v, pick_v, pull_hi_v, pull_lo_v, msg_v, rows_v, part_v, red_v, back_v, home_v, last_v, resid_v, total_v,
    load_sem, mix_send, mix_recv, out_send, self_send, in_recv, gat_send, gat_recv,
    red_send, red_recv, ret_send, ret_recv, last_send, last_recv,
):
    f32, bf16 = jnp.float32, jnp.bfloat16
    seqs, width = tokens_v.shape
    pieces = width // LANES
    slots = 2 * nz
    per = slots // CHUNKS
    experts = nz * NX * 2

    me = lax.axis_index("ep")
    y = lax.axis_index("tp")
    c = me % 2
    x = (me // 2) % NX
    z = me // (2 * NX)
    px = (y + NX - x) % NX
    mine = px == x

    self_slot = z * 2 + c

    def partner(slot):
        return (slot // 2 * NX + px) * 2 + slot % 2

    far = sorted(range(nz), key=lambda off: -min(off, nz - off))
    around = [(z + off) % nz * 2 + (1 - c if other else c) for off in far for other in (1, 0)]

    def peer(step):
        return (y + step) % NY

    pairs = [
        (routes_h, routes_v), (weights_h, weights_v), (tokens_h, tokens_v), (gain_in_h, gain_in_v),
        (wq_h, wq_v), (wk_h, wk_v), (wv_h, wv_v), (wi_h, wi_v), (wf_h, wf_v),
        (scale_h, scale_v), (memory_h, memory_v), (head_gain_h, head_gain_v), (wo_h, wo_v),
        (gain_out_h, gain_out_v), (gain_ffn_h, gain_ffn_v), (eg_h, eg_v), (eu_h, eu_v), (ed_h, ed_v),
        (gain_last_h, gain_last_v),
    ]
    loads = {}
    for i, (src, dst) in enumerate(pairs):
        loads[id(dst)] = pltpu.make_async_copy(src, dst, load_sem.at[i])
        loads[id(dst)].start()

    def ready(*refs):
        for ref in refs:
            loads[id(ref)].wait()

    barrier = pltpu.get_barrier_semaphore()
    stays = [mine & (self_slot == slot) for slot in range(slots)]
    for step in range(1, NY):
        pl.semaphore_signal(barrier, inc=1, device_id=(me, peer(step)), device_id_type=MESH)
    for slot in around[:-1]:
        pl.semaphore_signal(barrier, inc=1, device_id=(partner(slot), y), device_id_type=MESH)

    @pl.when(jnp.logical_not(mine))
    def _():
        pl.semaphore_signal(barrier, inc=1, device_id=(partner(self_slot), y), device_id_type=MESH)

    ready(tokens_v, gain_in_v)
    xf = tokens_v[...].astype(f32)
    normed = (xf * rms(xf) * gain_in_v[...]).astype(bf16)
    ready(wq_v, wk_v, wv_v)
    key_dim = wq_v.shape[1]
    query = jnp.dot(normed, wq_v[...], preferred_element_type=f32) * key_dim ** (-0.5)
    keys = jnp.dot(normed, wk_v[...], preferred_element_type=f32)
    values = jnp.dot(normed, wv_v[...], preferred_element_type=f32)
    ready(wi_v, wf_v, scale_v)
    nf = normed.astype(f32)
    in_pre = jnp.sum(nf * wi_v[...].astype(f32), axis=-1, keepdims=True) + bi_s[0]
    fg = jnp.sum(nf * wf_v[...].astype(f32), axis=-1, keepdims=True) + bf_s[0]
    forget_log = jnp.minimum(fg, 0.0) - jnp.log1p(jnp.exp(-jnp.abs(fg)))
    tr = lax.broadcasted_iota(jnp.int32, (seqs, seqs), 0)
    tc = lax.broadcasted_iota(jnp.int32, (seqs, seqs), 1)
    log_scale = jnp.sum(
        jnp.where(tr == tc, jnp.broadcast_to(scale_v[...], (seqs, seqs)), 0.0), axis=-1, keepdims=True
    )
    carried = forget_log + log_scale
    new_max = jnp.maximum(carried, in_pre)
    carry_weight = jnp.exp(carried - new_max)
    fresh_weight = jnp.exp(in_pre - new_max)
    match = jnp.sum(query * keys, axis=-1, keepdims=True)
    turned = query.T
    ready(memory_v)
    for s in range(seqs):
        recall_v[s : s + 1, :] = jnp.sum(turned[:, s : s + 1] * memory_v[s], axis=0, keepdims=True)
    read = carry_weight * recall_v[...] + (fresh_weight * match) * values
    ready(head_gain_v, wo_v)
    headout = (read * rms(read) * head_gain_v[...]).astype(bf16)
    mix_v[y] = jnp.dot(headout, wo_v[...], preferred_element_type=f32).astype(bf16)

    pl.semaphore_wait(barrier, NY - 1 + slots - jnp.where(mine, 1, 0))

    def to_peers(ref, send_sem, recv_sem):
        copies = []
        for step in (2, 1, 3):
            copy = pltpu.make_async_remote_copy(
                src_ref=ref.at[y], dst_ref=ref.at[y], send_sem=send_sem.at[step], recv_sem=recv_sem.at[step],
                device_id=(me, peer(step)), device_id_type=MESH,
            )
            copy.start()
            copies.append(copy)
        return copies

    def from_peers(ref, send_sem, recv_sem):
        for step in range(1, NY):
            source = peer(NY - step)
            pltpu.make_async_remote_copy(
                src_ref=ref.at[source], dst_ref=ref.at[source], send_sem=send_sem.at[step],
                recv_sem=recv_sem.at[step], device_id=(me, peer(step)), device_id_type=MESH,
            ).wait_recv()

    mix_copies = to_peers(mix_v, mix_send, mix_recv)

    ready(routes_v, weights_v)
    expert_row = lax.broadcasted_iota(jnp.int32, (experts, seqs), 0)
    named = jnp.zeros((experts, seqs), f32)
    weight = jnp.zeros((experts, seqs), f32)
    for j in range(routes_v.shape[0]):
        hit = expert_row == routes_v[j : j + 1, :]
        named = jnp.where(hit, 1.0, named)
        weight = jnp.where(hit, weights_v[j : j + 1, :], weight)
    row = lax.broadcasted_iota(jnp.int32, (LANES, LANES), 0)
    col = lax.broadcasted_iota(jnp.int32, (LANES, LANES), 1)
    before = jnp.where(row[:seqs, :seqs] < col[:seqs, :seqs], 1.0, 0.0).astype(bf16)
    count = jnp.dot(named.astype(bf16), before, preferred_element_type=f32)
    first = jnp.where(count < 0.5, named, 0.0)
    second = named - first
    copies_of = jnp.where(row[:seqs] == col[:seqs] % seqs, 1.0, 0.0).astype(bf16)
    lines = slots * 2 * pieces
    r2 = lax.broadcasted_iota(jnp.int32, (lines, 2 * experts), 0)
    c2 = lax.broadcasted_iota(jnp.int32, (lines, 2 * experts), 1)
    goal = (r2 // (4 * pieces) * NX + px) * 2 + r2 // (2 * pieces) % 2
    choose = jnp.where(c2 == goal + r2 // pieces % 2 * experts, 1.0, 0.0).astype(bf16)
    r3 = lax.broadcasted_iota(jnp.int32, (lines, LANES), 0)
    c3 = lax.broadcasted_iota(jnp.int32, (lines, LANES), 1)
    same = (r3 % pieces) == (c3 // seqs)

    def spread(one, two):
        both = jnp.concatenate([one, two], axis=0).astype(bf16)
        wide = jnp.dot(both, copies_of, preferred_element_type=f32).astype(bf16)
        return jnp.where(same, jnp.dot(choose, wide, preferred_element_type=f32), 0.0)

    pick_v[...] = spread(first, second).astype(bf16)

    from_peers(mix_v, mix_send, mix_recv)
    mixed = mix_v[0].astype(f32)
    for i in range(1, NY):
        mixed = mixed + mix_v[i].astype(f32)
    ready(gain_out_v, gain_ffn_v)
    resid = (xf + mixed * rms(mixed) * gain_out_v[...]).astype(bf16)
    rf = resid.astype(f32)
    resid_v[...] = rf
    ffn_in = (rf * rms(rf) * gain_ffn_v[...]).astype(bf16)

    def stacked(array):
        return jnp.concatenate([array[:, k * LANES : (k + 1) * LANES] for k in range(pieces)], axis=0)

    message = jnp.dot(pick_v[...], stacked(ffn_in), preferred_element_type=f32).astype(bf16)
    msg_v[...] = message.reshape(slots, 2 * pieces, LANES)

    def away(slot, src, dst, send_sem, recv_sem):
        return pltpu.make_async_remote_copy(
            src_ref=src, dst_ref=dst, send_sem=send_sem, recv_sem=recv_sem,
            device_id=(partner(slot), y), device_id_type=MESH,
        )

    own = away(self_slot, msg_v.at[self_slot], rows_v.at[y, self_slot], self_send, in_recv.at[self_slot])
    @pl.when(mine)
    def _():
        rows_v[y, self_slot] = msg_v[self_slot]

    for slot in around[:-1]:
        away(slot, msg_v.at[slot], rows_v.at[y, self_slot], out_send, in_recv.at[self_slot]).start()

    @pl.when(jnp.logical_not(mine))
    def _():
        own.start()

    hi = weight.astype(bf16).astype(f32)
    lo = weight - hi
    pull_hi_v[...] = spread(first * hi, second * hi).T.astype(bf16)
    pull_lo_v[...] = spread(first * lo, second * lo).T.astype(bf16)

    half = 2 * per
    row = lax.broadcasted_iota(jnp.int32, (half * pieces, half * pieces), 0)
    col = lax.broadcasted_iota(jnp.int32, (half * pieces, half * pieces), 1)
    order = jnp.where((row // half == col % pieces) & (row % half == col // pieces), 1.0, 0.0).astype(bf16)
    disorder = jnp.where((col // half == row % pieces) & (col % half == row // pieces), 1.0, 0.0).astype(bf16)

    ready(eg_v, eu_v, ed_v)

    def from_afar(slot, ref, send_sem, recv_sem):
        @pl.when(jnp.logical_not(stays[slot]))
        def _():
            away(slot, ref, ref, send_sem, recv_sem.at[slot]).wait_recv()

    def arrive(g):
        for slot in range(g * per, (g + 1) * per):
            from_afar(slot, rows_v.at[y, slot], out_send, in_recv)
        for step in range(1, NY):
            piece = rows_v.at[y, pl.ds(g * per, per)]
            pltpu.make_async_remote_copy(
                src_ref=piece, dst_ref=piece, send_sem=gat_send, recv_sem=gat_recv.at[step, g],
                device_id=(me, peer(step)), device_id_type=MESH,
            ).start()

    def expert(g):
        for step in range(1, NY):
            source = peer(NY - step)
            piece = rows_v.at[source, pl.ds(g * per, per)]
            pltpu.make_async_remote_copy(
                src_ref=piece, dst_ref=piece, send_sem=gat_send, recv_sem=gat_recv.at[step, g],
                device_id=(me, peer(step)), device_id_type=MESH,
            ).wait_recv()
        side = jnp.concatenate(
            [rows_v[i, g * per : (g + 1) * per].reshape(per * 2 * pieces, LANES) for i in range(NY)], axis=1
        )
        sorted_rows = jnp.dot(order, side, preferred_element_type=f32).astype(bf16)
        inputs = jnp.concatenate(
            [
                jnp.concatenate(
                    [sorted_rows[k * half : (k + 1) * half, i * LANES : (i + 1) * LANES] for k in range(pieces)],
                    axis=1,
                )
                for i in range(NY)
            ],
            axis=0,
        )
        gate = jnp.dot(inputs, eg_v[...], preferred_element_type=f32)
        up = jnp.dot(inputs, eu_v[...], preferred_element_type=f32)
        act = (jax.nn.silu(gate) * up).astype(bf16)
        part = jnp.dot(act, ed_v[...], preferred_element_type=f32).astype(bf16)
        for i in range(NY):
            part_v[g, i] = part[i * half : (i + 1) * half, :]
        for step in range(1, NY):
            pltpu.make_async_remote_copy(
                src_ref=part_v.at[g, peer(step)], dst_ref=red_v.at[g, step], send_sem=red_send,
                recv_sem=red_recv.at[step, g], device_id=(me, peer(step)), device_id_type=MESH,
            ).start()

    def give_back(g):
        total = part_v[g, y].astype(f32)
        for step in range(1, NY):
            pltpu.make_async_remote_copy(
                src_ref=part_v.at[g, peer(step)], dst_ref=red_v.at[g, step], send_sem=red_send,
                recv_sem=red_recv.at[step, g], device_id=(me, peer(step)), device_id_type=MESH,
            ).wait_recv()
        for step in range(1, NY):
            total = total + red_v[g, step].astype(f32)
        lined = jnp.dot(disorder, stacked(total.astype(bf16)), preferred_element_type=f32).astype(bf16)
        back_v[g * per : (g + 1) * per] = lined.reshape(per, 2 * pieces, LANES)
        for slot in range(g * per, (g + 1) * per):
            @pl.when(jnp.logical_not(stays[slot]))
            def _():
                away(slot, back_v.at[slot], home_v.at[self_slot], ret_send, ret_recv.at[self_slot]).start()

            @pl.when(stays[slot])
            def _():
                home_v[slot] = back_v[slot]

    for g in ORDER:
        arrive(g)
    for g in ORDER:
        expert(g)
    for g in ORDER:
        give_back(g)

    routed = jnp.zeros((LANES, LANES), f32)
    for g in ORDER:
        for slot in range(g * per, (g + 1) * per):
            from_afar(slot, home_v.at[slot], ret_send, ret_recv)
        block = home_v[g * per : (g + 1) * per].reshape(per * 2 * pieces, LANES)
        span = slice(g * per * 2 * pieces, (g + 1) * per * 2 * pieces)
        routed = routed + jnp.dot(pull_hi_v[:, span], block, preferred_element_type=f32)
        routed = routed + jnp.dot(pull_lo_v[:, span], block, preferred_element_type=f32)
    flat = jnp.concatenate([routed[k * seqs : (k + 1) * seqs, :] for k in range(pieces)], axis=1)
    last_v[y] = flat.astype(bf16)
    last_copies = to_peers(last_v, last_send, last_recv)
    from_peers(last_v, last_send, last_recv)
    total = last_v[0].astype(f32)
    for i in range(1, NY):
        total = total + last_v[i].astype(f32)
    total_v[...] = total * rms(total)
    ready(gain_last_v)
    quarter = width // NY
    mark = pl.ds(pl.multiple_of(y * quarter, quarter), quarter)
    out_ref[...] = (resid_v[:, mark] + total_v[:, mark] * gain_last_v[...]).astype(bf16)

    for copy in mix_copies + last_copies:
        copy.wait_send()
    rest = msg_v.at[pl.ds(1, slots - 1)]
    away(self_slot, rest, rest, out_send, in_recv.at[0]).wait_send()
    away(self_slot, rest, rest, ret_send, ret_recv.at[0]).wait_send()

    @pl.when(jnp.logical_not(mine))
    def _():
        own.wait_send()
        away(self_slot, msg_v.at[0], msg_v.at[0], ret_send, ret_recv.at[0]).wait_send()

    everything = rows_v.at[pl.ds(0, NY - 1)]
    away(self_slot, everything, everything, gat_send, in_recv.at[0]).wait_send()
    everything = red_v.at[:, pl.ds(1, NY - 1)]
    away(self_slot, everything, everything, red_send, in_recv.at[0]).wait_send()


def per_device(
    nz, tokens, memory, log_scale, mix_gain_in, w_query, w_key, w_value, w_igate, w_fgate, igate_bias, fgate_bias,
    head_gain, w_output, mix_gain_out, ffn_gain_in, routes, route_weights, expert_gate, expert_up, expert_down,
    ffn_gain_out,
):
    f32, bf16 = jnp.float32, jnp.bfloat16
    seqs, width = tokens.shape
    pieces = width // LANES
    key_dim, value_dim = memory.shape[2:]
    slots = 2 * nz
    per = slots // CHUNKS
    lines = slots * 2 * pieces
    hidden = expert_gate.shape[2]
    operands = [
        tokens, memory[:, 0], log_scale.T, mix_gain_in[None], w_query, w_key, w_value, w_igate.T, w_fgate.T,
        igate_bias, fgate_bias, head_gain[None], w_output, mix_gain_out[None], ffn_gain_in[None],
        routes.T, route_weights.T,
        expert_gate[0], expert_up[0], expert_down[0], ffn_gain_out[None],
    ]
    dma, vmem = pltpu.SemaphoreType.DMA, pltpu.VMEM
    scratch = [vmem(a.shape, a.dtype) for a in operands if a.size > 1] + [
        vmem((seqs, value_dim), f32),
        vmem((NY, seqs, width), bf16),
        vmem((lines, LANES), bf16),
        vmem((LANES, lines), bf16),
        vmem((LANES, lines), bf16),
        vmem((slots, 2 * pieces, LANES), bf16),
        vmem((NY, slots, 2 * pieces, LANES), bf16),
        vmem((CHUNKS, NY, 2 * per, width), bf16),
        vmem((CHUNKS, NY, 2 * per, width), bf16),
        vmem((slots, 2 * pieces, LANES), bf16),
        vmem((slots, 2 * pieces, LANES), bf16),
        vmem((NY, seqs, width), bf16),
        vmem((seqs, width), f32),
        vmem((seqs, width), f32),
        dma((len(operands),)), dma((NY,)), dma((NY,)), dma, dma, dma((slots,)), dma, dma((NY, CHUNKS)),
        dma, dma((NY, CHUNKS)), dma, dma((slots,)), dma((NY,)), dma((NY,)),
    ]
    return pl.pallas_call(
        functools.partial(kernel, nz),
        out_shape=jax.ShapeDtypeStruct((seqs, width // NY), bf16),
        in_specs=[pl.BlockSpec(memory_space=pltpu.HBM if a.size > 1 else pltpu.SMEM) for a in operands],
        out_specs=pl.BlockSpec(memory_space=pltpu.VMEM),
        scratch_shapes=scratch,
        compiler_params=pltpu.CompilerParams(collective_id=0, has_side_effects=True, vmem_limit_bytes=67043328),
    )(*operands)


def solution(mesh):
    nz = mesh.shape["ep"] // (2 * NX)
    return jax.shard_map(
        functools.partial(per_device, nz),
        mesh=mesh,
        in_specs=(
            P("ep", None), P("ep", "tp", None, None), P("ep", "tp"), P(), P(None, "tp"), P(None, "tp"),
            P(None, "tp"), P(None, "tp"), P(None, "tp"), P("tp"), P("tp"), P("tp"), P("tp", None), P(), P(),
            P("ep", None), P("ep", None), P("ep", None, "tp"), P("ep", None, "tp"), P("ep", "tp", None), P("tp"),
        ),
        out_specs=P("ep", "tp"),
        check_vma=False,
    )
```

```python
import functools

import jax
import jax.numpy as jnp
from jax import lax
from jax.experimental import pallas as pl
from jax.experimental.pallas import tpu as pltpu
from jax.sharding import PartitionSpec as P

EPS = 1e-06
MESH = pl.DeviceIdType.MESH
LANES = 128
NX = 4
NY = 4
CHUNKS = 4
VMEM_LIMIT = 67043328 - 65536
TURNS = ((0, 1, 3, 2), (0, 1, 3, 2), (2, 3, 0, 1), (3, 2, 0, 1))


def rms(values):
    return lax.rsqrt(jnp.mean(values * values, axis=-1, keepdims=True) + EPS)


def kernel(
    nz,
    tokens_h, memory_h, scale_h, gain_in_h, wq_h, wk_h, wv_h, wi_h, wf_h, bi_s, bf_s,
    head_gain_h, wo_h, gain_out_h, gain_ffn_h, routes_h, weights_h, eg_h, eu_h, ed_h, gain_last_h,
    out_ref,
    tokens_v, memory_v, scale_v, gain_in_v, wq_v, wk_v, wv_v, wi_v, wf_v,
    head_gain_v, wo_v, gain_out_v, gain_ffn_v, routes_v, weights_v, eg_v, eu_v, ed_v, gain_last_v,
    recall_v, mix_v, pick_v, pull_hi_v, pull_lo_v, msg_v, rows_v, part_v, red_v, back_v, home_v, last_v, resid_v, total_v,
    load_sem, mix_send, mix_recv, out_send, self_send, in_recv, gat_send, gat_recv,
    red_send, red_recv, ret_send, ret_recv, last_send, last_recv,
):
    f32, bf16 = jnp.float32, jnp.bfloat16
    seqs, width = tokens_v.shape
    pieces = width // LANES
    slots = 2 * nz
    per = slots // CHUNKS
    experts = nz * NX * 2

    me = lax.axis_index("ep")
    y = lax.axis_index("tp")
    c = me % 2
    x = (me // 2) % NX
    z = me // (2 * NX)
    px = (y + NX - x) % NX
    mine = px == x

    self_slot = z * 2 + c

    def partner(slot):
        return (slot // 2 * NX + px) * 2 + slot % 2

    far = sorted(range(nz), key=lambda off: -min(off, nz - off))
    around = [(z + off) % nz * 2 + (1 - c if other else c) for off in far for other in (1, 0)]

    def peer(step):
        return (y + step) % NY

    pairs = [
        (routes_h, routes_v), (weights_h, weights_v), (tokens_h, tokens_v), (gain_in_h, gain_in_v),
        (wq_h, wq_v), (wk_h, wk_v), (wv_h, wv_v), (wi_h, wi_v), (wf_h, wf_v),
        (scale_h, scale_v), (memory_h, memory_v), (head_gain_h, head_gain_v), (wo_h, wo_v),
        (gain_out_h, gain_out_v), (gain_ffn_h, gain_ffn_v), (eg_h, eg_v), (eu_h, eu_v), (ed_h, ed_v),
        (gain_last_h, gain_last_v),
    ]
    loads = {}
    for i, (src, dst) in enumerate(pairs):
        loads[id(dst)] = pltpu.make_async_copy(src, dst, load_sem.at[i])
        loads[id(dst)].start()

    def ready(*refs):
        for ref in refs:
            loads[id(ref)].wait()

    barrier = pltpu.get_barrier_semaphore()
    for step in range(1, NY):
        pl.semaphore_signal(barrier, inc=1, device_id=(me, peer(step)), device_id_type=MESH)
    for slot in around[:-1]:
        pl.semaphore_signal(barrier, inc=1, device_id=(partner(slot), y), device_id_type=MESH)

    @pl.when(jnp.logical_not(mine))
    def _():
        pl.semaphore_signal(barrier, inc=1, device_id=(partner(self_slot), y), device_id_type=MESH)

    ready(tokens_v, gain_in_v)
    xf = tokens_v[...].astype(f32)
    normed = (xf * rms(xf) * gain_in_v[...]).astype(bf16)
    ready(wq_v, wk_v, wv_v)
    key_dim = wq_v.shape[1]
    query = jnp.dot(normed, wq_v[...], preferred_element_type=f32) * key_dim ** (-0.5)
    keys = jnp.dot(normed, wk_v[...], preferred_element_type=f32)
    values = jnp.dot(normed, wv_v[...], preferred_element_type=f32)
    ready(wi_v, wf_v, scale_v)
    nf = normed.astype(f32)
    in_pre = jnp.sum(nf * wi_v[...].astype(f32), axis=-1, keepdims=True) + bi_s[0]
    fg = jnp.sum(nf * wf_v[...].astype(f32), axis=-1, keepdims=True) + bf_s[0]
    forget_log = jnp.minimum(fg, 0.0) - jnp.log1p(jnp.exp(-jnp.abs(fg)))
    tr = lax.broadcasted_iota(jnp.int32, (seqs, seqs), 0)
    tc = lax.broadcasted_iota(jnp.int32, (seqs, seqs), 1)
    log_scale = jnp.sum(
        jnp.where(tr == tc, jnp.broadcast_to(scale_v[...], (seqs, seqs)), 0.0), axis=-1, keepdims=True
    )
    carried = forget_log + log_scale
    new_max = jnp.maximum(carried, in_pre)
    carry_weight = jnp.exp(carried - new_max)
    fresh_weight = jnp.exp(in_pre - new_max)
    match = jnp.sum(query * keys, axis=-1, keepdims=True)
    turned = query.T
    ready(memory_v)
    for s in range(seqs):
        recall_v[s : s + 1, :] = jnp.sum(turned[:, s : s + 1] * memory_v[s], axis=0, keepdims=True)
    read = carry_weight * recall_v[...] + (fresh_weight * match) * values
    ready(head_gain_v, wo_v)
    headout = (read * rms(read) * head_gain_v[...]).astype(bf16)
    mix_v[y] = jnp.dot(headout, wo_v[...], preferred_element_type=f32).astype(bf16)

    pl.semaphore_wait(barrier, NY - 1 + slots - jnp.where(mine, 1, 0))

    def to_peers(ref, send_sem, recv_sem):
        copies = []
        for step in (2, 1, 3):
            copy = pltpu.make_async_remote_copy(
                src_ref=ref.at[y], dst_ref=ref.at[y], send_sem=send_sem.at[step], recv_sem=recv_sem.at[step],
                device_id=(me, peer(step)), device_id_type=MESH,
            )
            copy.start()
            copies.append(copy)
        return copies

    def from_peers(ref, send_sem, recv_sem):
        for step in range(1, NY):
            source = peer(NY - step)
            pltpu.make_async_remote_copy(
                src_ref=ref.at[source], dst_ref=ref.at[source], send_sem=send_sem.at[step],
                recv_sem=recv_sem.at[step], device_id=(me, peer(step)), device_id_type=MESH,
            ).wait_recv()

    mix_copies = to_peers(mix_v, mix_send, mix_recv)

    ready(routes_v, weights_v)
    expert_row = lax.broadcasted_iota(jnp.int32, (experts, seqs), 0)
    named = jnp.zeros((experts, seqs), f32)
    weight = jnp.zeros((experts, seqs), f32)
    for j in range(routes_v.shape[0]):
        hit = expert_row == routes_v[j : j + 1, :]
        named = jnp.where(hit, 1.0, named)
        weight = jnp.where(hit, weights_v[j : j + 1, :], weight)
    row = lax.broadcasted_iota(jnp.int32, (LANES, LANES), 0)
    col = lax.broadcasted_iota(jnp.int32, (LANES, LANES), 1)
    before = jnp.where(row[:seqs, :seqs] < col[:seqs, :seqs], 1.0, 0.0).astype(bf16)
    count = jnp.dot(named.astype(bf16), before, preferred_element_type=f32)
    first = jnp.where(count < 0.5, named, 0.0)
    second = named - first
    copies_of = jnp.where(row[:seqs] == col[:seqs] % seqs, 1.0, 0.0).astype(bf16)
    lines = slots * 2 * pieces
    r2 = lax.broadcasted_iota(jnp.int32, (lines, 2 * experts), 0)
    c2 = lax.broadcasted_iota(jnp.int32, (lines, 2 * experts), 1)
    goal = (r2 // (4 * pieces) * NX + px) * 2 + r2 // (2 * pieces) % 2
    choose = jnp.where(c2 == goal + r2 // pieces % 2 * experts, 1.0, 0.0).astype(bf16)
    r3 = lax.broadcasted_iota(jnp.int32, (lines, LANES), 0)
    c3 = lax.broadcasted_iota(jnp.int32, (lines, LANES), 1)
    same = (r3 % pieces) == (c3 // seqs)

    def spread(one, two):
        both = jnp.concatenate([one, two], axis=0).astype(bf16)
        wide = jnp.dot(both, copies_of, preferred_element_type=f32).astype(bf16)
        return jnp.where(same, jnp.dot(choose, wide, preferred_element_type=f32), 0.0)

    pick_v[...] = spread(first, second).astype(bf16)

    from_peers(mix_v, mix_send, mix_recv)
    mixed = mix_v[0].astype(f32)
    for i in range(1, NY):
        mixed = mixed + mix_v[i].astype(f32)
    ready(gain_out_v, gain_ffn_v)
    resid = (xf + mixed * rms(mixed) * gain_out_v[...]).astype(bf16)
    rf = resid.astype(f32)
    resid_v[...] = rf
    ffn_in = (rf * rms(rf) * gain_ffn_v[...]).astype(bf16)

    def stacked(array):
        return jnp.concatenate([array[:, k * LANES : (k + 1) * LANES] for k in range(pieces)], axis=0)

    message = jnp.dot(pick_v[...], stacked(ffn_in), preferred_element_type=f32).astype(bf16)
    msg_v[...] = message.reshape(slots, 2 * pieces, LANES)

    def away(slot, src, dst, send_sem, recv_sem):
        return pltpu.make_async_remote_copy(
            src_ref=src, dst_ref=dst, send_sem=send_sem, recv_sem=recv_sem,
            device_id=(partner(slot), y), device_id_type=MESH,
        )

    own = away(self_slot, msg_v.at[self_slot], rows_v.at[y, self_slot], self_send, in_recv.at[self_slot])
    @pl.when(mine)
    def _():
        rows_v[y, self_slot] = msg_v[self_slot]

    for slot in around[:-1]:
        away(slot, msg_v.at[slot], rows_v.at[y, self_slot], out_send, in_recv.at[self_slot]).start()

    @pl.when(jnp.logical_not(mine))
    def _():
        own.start()

    hi = weight.astype(bf16).astype(f32)
    lo = weight - hi
    pull_hi_v[...] = spread(first * hi, second * hi).T.astype(bf16)
    pull_lo_v[...] = spread(first * lo, second * lo).T.astype(bf16)

    half = 2 * per
    row = lax.broadcasted_iota(jnp.int32, (half * pieces, half * pieces), 0)
    col = lax.broadcasted_iota(jnp.int32, (half * pieces, half * pieces), 1)
    order = jnp.where((row // half == col % pieces) & (row % half == col // pieces), 1.0, 0.0).astype(bf16)
    disorder = jnp.where((col // half == row % pieces) & (col % half == row // pieces), 1.0, 0.0).astype(bf16)

    ready(eg_v, eu_v, ed_v)

    def from_afar(slot, ref, send_sem, recv_sem):
        @pl.when(jnp.logical_not(mine & (self_slot == slot)))
        def _():
            away(slot, ref, ref, send_sem, recv_sem.at[slot]).wait_recv()

    def arrive(g):
        for slot in [g * per + i for i in range(per)]:
            from_afar(slot, rows_v.at[y, slot], out_send, in_recv)
        for step in range(1, NY):
            piece = rows_v.at[y, pl.ds(g * per, per)]
            pltpu.make_async_remote_copy(
                src_ref=piece, dst_ref=piece, send_sem=gat_send, recv_sem=gat_recv.at[step, g],
                device_id=(me, peer(step)), device_id_type=MESH,
            ).start()

    def expert(g):
        for step in range(1, NY):
            source = peer(NY - step)
            piece = rows_v.at[source, pl.ds(g * per, per)]
            pltpu.make_async_remote_copy(
                src_ref=piece, dst_ref=piece, send_sem=gat_send, recv_sem=gat_recv.at[step, g],
                device_id=(me, peer(step)), device_id_type=MESH,
            ).wait_recv()
        side = jnp.concatenate(
            [rows_v[i, pl.ds(g * per, per)].reshape(per * 2 * pieces, LANES) for i in range(NY)], axis=1
        )
        sorted_rows = jnp.dot(order, side, preferred_element_type=f32).astype(bf16)
        inputs = jnp.concatenate(
            [
                jnp.concatenate(
                    [sorted_rows[k * half : (k + 1) * half, i * LANES : (i + 1) * LANES] for k in range(pieces)],
                    axis=1,
                )
                for i in range(NY)
            ],
            axis=0,
        )
        gate = jnp.dot(inputs, eg_v[...], preferred_element_type=f32)
        up = jnp.dot(inputs, eu_v[...], preferred_element_type=f32)
        act = (jax.nn.silu(gate) * up).astype(bf16)
        part = jnp.dot(act, ed_v[...], preferred_element_type=f32).astype(bf16)
        for i in range(NY):
            part_v[g, i] = part[i * half : (i + 1) * half, :]
        for step in range(1, NY):
            pltpu.make_async_remote_copy(
                src_ref=part_v.at[g, peer(step)], dst_ref=red_v.at[g, step], send_sem=red_send,
                recv_sem=red_recv.at[step, g], device_id=(me, peer(step)), device_id_type=MESH,
            ).start()

    def give_back(g):
        total = part_v[g, y].astype(f32)
        for step in range(1, NY):
            pltpu.make_async_remote_copy(
                src_ref=part_v.at[g, peer(step)], dst_ref=red_v.at[g, step], send_sem=red_send,
                recv_sem=red_recv.at[step, g], device_id=(me, peer(step)), device_id_type=MESH,
            ).wait_recv()
        for step in range(1, NY):
            total = total + red_v[g, step].astype(f32)
        lined = jnp.dot(disorder, stacked(total.astype(bf16)), preferred_element_type=f32).astype(bf16)
        back_v[pl.ds(g * per, per)] = lined.reshape(per, 2 * pieces, LANES)
        for slot in [g * per + i for i in range(per)]:
            here = mine & (self_slot == slot)

            @pl.when(jnp.logical_not(here))
            def _():
                away(slot, back_v.at[slot], home_v.at[self_slot], ret_send, ret_recv.at[self_slot]).start()

            @pl.when(here)
            def _():
                home_v[slot] = back_v[slot]

    group = z // (nz // CHUNKS)
    turn = [sum(jnp.where(group == k, order_k[i], 0) for k, order_k in enumerate(TURNS)) for i in range(CHUNKS)]
    for g in turn:
        arrive(g)
    for g in turn:
        expert(g)
    for g in turn:
        give_back(g)

    routed = jnp.zeros((LANES, LANES), f32)
    for g in range(CHUNKS):
        for slot in range(g * per, (g + 1) * per):
            from_afar(slot, home_v.at[slot], ret_send, ret_recv)
        block = home_v[g * per : (g + 1) * per].reshape(per * 2 * pieces, LANES)
        span = slice(g * per * 2 * pieces, (g + 1) * per * 2 * pieces)
        routed = routed + jnp.dot(pull_hi_v[:, span], block, preferred_element_type=f32)
        routed = routed + jnp.dot(pull_lo_v[:, span], block, preferred_element_type=f32)
    flat = jnp.concatenate([routed[k * seqs : (k + 1) * seqs, :] for k in range(pieces)], axis=1)
    last_v[y] = flat.astype(bf16)
    last_copies = to_peers(last_v, last_send, last_recv)
    from_peers(last_v, last_send, last_recv)
    total = last_v[0].astype(f32)
    for i in range(1, NY):
        total = total + last_v[i].astype(f32)
    total_v[...] = total * rms(total)
    ready(gain_last_v)
    quarter = width // NY
    mark = pl.ds(pl.multiple_of(y * quarter, quarter), quarter)
    out_ref[...] = (resid_v[:, mark] + total_v[:, mark] * gain_last_v[...]).astype(bf16)

    for copy in mix_copies + last_copies:
        copy.wait_send()
    rest = msg_v.at[pl.ds(1, slots - 1)]
    away(self_slot, rest, rest, out_send, in_recv.at[0]).wait_send()
    away(self_slot, rest, rest, ret_send, ret_recv.at[0]).wait_send()

    @pl.when(jnp.logical_not(mine))
    def _():
        own.wait_send()
        away(self_slot, msg_v.at[0], msg_v.at[0], ret_send, ret_recv.at[0]).wait_send()

    everything = rows_v.at[pl.ds(0, NY - 1)]
    away(self_slot, everything, everything, gat_send, in_recv.at[0]).wait_send()
    everything = red_v.at[:, pl.ds(1, NY - 1)]
    away(self_slot, everything, everything, red_send, in_recv.at[0]).wait_send()


def per_device(
    nz, tokens, memory, log_scale, mix_gain_in, w_query, w_key, w_value, w_igate, w_fgate, igate_bias, fgate_bias,
    head_gain, w_output, mix_gain_out, ffn_gain_in, routes, route_weights, expert_gate, expert_up, expert_down,
    ffn_gain_out,
):
    f32, bf16 = jnp.float32, jnp.bfloat16
    seqs, width = tokens.shape
    pieces = width // LANES
    key_dim, value_dim = memory.shape[2:]
    slots = 2 * nz
    per = slots // CHUNKS
    lines = slots * 2 * pieces
    hidden = expert_gate.shape[2]
    operands = [
        tokens, memory[:, 0], log_scale.T, mix_gain_in[None], w_query, w_key, w_value, w_igate.T, w_fgate.T,
        igate_bias, fgate_bias, head_gain[None], w_output, mix_gain_out[None], ffn_gain_in[None],
        routes.T, route_weights.T,
        expert_gate[0], expert_up[0], expert_down[0], ffn_gain_out[None],
    ]
    dma, vmem = pltpu.SemaphoreType.DMA, pltpu.VMEM
    scratch = [vmem(a.shape, a.dtype) for a in operands if a.size > 1] + [
        vmem((seqs, value_dim), f32),
        vmem((NY, seqs, width), bf16),
        vmem((lines, LANES), bf16),
        vmem((LANES, lines), bf16),
        vmem((LANES, lines), bf16),
        vmem((slots, 2 * pieces, LANES), bf16),
        vmem((NY, slots, 2 * pieces, LANES), bf16),
        vmem((CHUNKS, NY, 2 * per, width), bf16),
        vmem((CHUNKS, NY, 2 * per, width), bf16),
        vmem((slots, 2 * pieces, LANES), bf16),
        vmem((slots, 2 * pieces, LANES), bf16),
        vmem((NY, seqs, width), bf16),
        vmem((seqs, width), f32),
        vmem((seqs, width), f32),
        dma((len(operands),)), dma((NY,)), dma((NY,)), dma, dma, dma((slots,)), dma, dma((NY, CHUNKS)),
        dma, dma((NY, CHUNKS)), dma, dma((slots,)), dma((NY,)), dma((NY,)),
    ]
    return pl.pallas_call(
        functools.partial(kernel, nz),
        out_shape=vmem((seqs, width // NY), bf16),
        in_specs=[pl.BlockSpec(memory_space=pltpu.HBM if a.size > 1 else pltpu.SMEM) for a in operands],
        out_specs=pl.BlockSpec(memory_space=pltpu.VMEM),
        scratch_shapes=scratch,
        compiler_params=pltpu.CompilerParams(collective_id=0, has_side_effects=True, vmem_limit_bytes=VMEM_LIMIT),
    )(*operands)


def solution(mesh):
    nz = mesh.shape["ep"] // (2 * NX)
    return jax.shard_map(
        functools.partial(per_device, nz),
        mesh=mesh,
        in_specs=(
            P("ep", None), P("ep", "tp", None, None), P("ep", "tp"), P(), P(None, "tp"), P(None, "tp"),
            P(None, "tp"), P(None, "tp"), P(None, "tp"), P("tp"), P("tp"), P("tp"), P("tp", None), P(), P(),
            P("ep", None), P("ep", None), P("ep", None, "tp"), P("ep", None, "tp"), P("ep", "tp", None), P("tp"),
        ),
        out_specs=P("ep", "tp"),
        check_vma=False,
    )
```

```python
import functools

import jax
import jax.numpy as jnp
from jax import lax
from jax.experimental import pallas as pl
from jax.experimental.pallas import tpu as pltpu
from jax.sharding import PartitionSpec as P

EPS = 1e-06
MESH = pl.DeviceIdType.MESH
LANES = 128
NX = 4
NY = 4
CHUNKS = 4
VMEM_LIMIT = 67043328 - 65536
TURNS = ((0, 1, 3, 2), (0, 1, 3, 2), (2, 3, 0, 1), (3, 2, 0, 1))


def rms(values):
    return lax.rsqrt(jnp.mean(values * values, axis=-1, keepdims=True) + EPS)


def kernel(
    nz,
    tokens_h, memory_h, scale_h, gain_in_h, wq_h, wk_h, wv_h, wi_h, wf_h, bi_s, bf_s,
    head_gain_h, wo_h, gain_out_h, gain_ffn_h, routes_h, weights_h, eg_h, eu_h, ed_h, gain_last_h,
    out_ref,
    tokens_v, memory_v, scale_v, gain_in_v, wq_v, wk_v, wv_v, wi_v, wf_v,
    head_gain_v, wo_v, gain_out_v, gain_ffn_v, routes_v, weights_v, eg_v, eu_v, ed_v, gain_last_v,
    recall_v, mix_v, pick_v, pull_hi_v, pull_lo_v, msg_v, rows_v, part_v, red_v, back_v, home_v, last_v, resid_v, total_v,
    load_sem, mix_send, mix_recv, out_send, self_send, in_recv, gat_send, gat_recv,
    red_send, red_recv, ret_send, ret_recv, last_send, last_recv,
):
    f32, bf16 = jnp.float32, jnp.bfloat16
    seqs, width = tokens_v.shape
    pieces = width // LANES
    slots = 2 * nz
    per = slots // CHUNKS
    experts = nz * NX * 2

    me = lax.axis_index("ep")
    y = lax.axis_index("tp")
    c = me % 2
    x = (me // 2) % NX
    z = me // (2 * NX)
    px = (y + NX - x) % NX
    mine = px == x

    self_slot = z * 2 + c

    def partner(slot):
        return (slot // 2 * NX + px) * 2 + slot % 2

    far = sorted(range(nz), key=lambda off: -min(off, nz - off))
    around = [(z + off) % nz * 2 + (1 - c if other else c) for off in far for other in (1, 0)]

    def peer(step):
        return (y + step) % NY

    pairs = [
        (routes_h, routes_v), (weights_h, weights_v), (tokens_h, tokens_v), (gain_in_h, gain_in_v),
        (wq_h, wq_v), (wk_h, wk_v), (wv_h, wv_v), (wi_h, wi_v), (wf_h, wf_v),
        (scale_h, scale_v), (memory_h, memory_v), (head_gain_h, head_gain_v), (wo_h, wo_v),
        (gain_out_h, gain_out_v), (gain_ffn_h, gain_ffn_v), (eg_h, eg_v), (eu_h, eu_v), (ed_h, ed_v),
        (gain_last_h, gain_last_v),
    ]
    loads = {}
    for i, (src, dst) in enumerate(pairs):
        loads[id(dst)] = pltpu.make_async_copy(src, dst, load_sem.at[i])
        loads[id(dst)].start()

    def ready(*refs):
        for ref in refs:
            loads[id(ref)].wait()

    barrier = pltpu.get_barrier_semaphore()
    for step in range(1, NY):
        pl.semaphore_signal(barrier, inc=1, device_id=(me, peer(step)), device_id_type=MESH)
    for slot in around[:-1]:
        pl.semaphore_signal(barrier, inc=1, device_id=(partner(slot), y), device_id_type=MESH)

    @pl.when(jnp.logical_not(mine))
    def _():
        pl.semaphore_signal(barrier, inc=1, device_id=(partner(self_slot), y), device_id_type=MESH)

    ready(tokens_v, gain_in_v)
    xf = tokens_v[...].astype(f32)
    normed = (xf * rms(xf) * gain_in_v[...]).astype(bf16)
    ready(wq_v, wk_v, wv_v)
    key_dim = wq_v.shape[1]
    query = jnp.dot(normed, wq_v[...], preferred_element_type=f32) * key_dim ** (-0.5)
    keys = jnp.dot(normed, wk_v[...], preferred_element_type=f32)
    values = jnp.dot(normed, wv_v[...], preferred_element_type=f32)
    ready(wi_v, wf_v, scale_v)
    nf = normed.astype(f32)
    in_pre = jnp.sum(nf * wi_v[...].astype(f32), axis=-1, keepdims=True) + bi_s[0]
    fg = jnp.sum(nf * wf_v[...].astype(f32), axis=-1, keepdims=True) + bf_s[0]
    forget_log = jnp.minimum(fg, 0.0) - jnp.log1p(jnp.exp(-jnp.abs(fg)))
    tr = lax.broadcasted_iota(jnp.int32, (seqs, seqs), 0)
    tc = lax.broadcasted_iota(jnp.int32, (seqs, seqs), 1)
    log_scale = jnp.sum(
        jnp.where(tr == tc, jnp.broadcast_to(scale_v[...], (seqs, seqs)), 0.0), axis=-1, keepdims=True
    )
    carried = forget_log + log_scale
    new_max = jnp.maximum(carried, in_pre)
    carry_weight = jnp.exp(carried - new_max)
    fresh_weight = jnp.exp(in_pre - new_max)
    match = jnp.sum(query * keys, axis=-1, keepdims=True)
    turned = query.T
    ready(memory_v)
    for s in range(seqs):
        recall_v[s : s + 1, :] = jnp.sum(turned[:, s : s + 1] * memory_v[s], axis=0, keepdims=True)
    read = carry_weight * recall_v[...] + (fresh_weight * match) * values
    ready(head_gain_v, wo_v)
    headout = (read * rms(read) * head_gain_v[...]).astype(bf16)
    mix_v[y] = jnp.dot(headout, wo_v[...], preferred_element_type=f32).astype(bf16)

    pl.semaphore_wait(barrier, NY - 1 + slots - jnp.where(mine, 1, 0))

    def to_peers(ref, send_sem, recv_sem):
        copies = []
        for step in (2, 1, 3):
            copy = pltpu.make_async_remote_copy(
                src_ref=ref.at[y], dst_ref=ref.at[y], send_sem=send_sem.at[step], recv_sem=recv_sem.at[step],
                device_id=(me, peer(step)), device_id_type=MESH,
            )
            copy.start()
            copies.append(copy)
        return copies

    def from_peers(ref, send_sem, recv_sem):
        for step in range(1, NY):
            source = peer(NY - step)
            pltpu.make_async_remote_copy(
                src_ref=ref.at[source], dst_ref=ref.at[source], send_sem=send_sem.at[step],
                recv_sem=recv_sem.at[step], device_id=(me, peer(step)), device_id_type=MESH,
            ).wait_recv()

    mix_copies = to_peers(mix_v, mix_send, mix_recv)

    ready(routes_v, weights_v)
    expert_row = lax.broadcasted_iota(jnp.int32, (experts, seqs), 0)
    named = jnp.zeros((experts, seqs), f32)
    weight = jnp.zeros((experts, seqs), f32)
    for j in range(routes_v.shape[0]):
        hit = expert_row == routes_v[j : j + 1, :]
        named = jnp.where(hit, 1.0, named)
        weight = jnp.where(hit, weights_v[j : j + 1, :], weight)
    row = lax.broadcasted_iota(jnp.int32, (LANES, LANES), 0)
    col = lax.broadcasted_iota(jnp.int32, (LANES, LANES), 1)
    before = jnp.where(row[:seqs, :seqs] < col[:seqs, :seqs], 1.0, 0.0).astype(bf16)
    count = jnp.dot(named.astype(bf16), before, preferred_element_type=f32)
    first = jnp.where(count < 0.5, named, 0.0)
    second = named - first
    copies_of = jnp.where(row[:seqs] == col[:seqs] % seqs, 1.0, 0.0).astype(bf16)
    lines = slots * 2 * pieces
    r2 = lax.broadcasted_iota(jnp.int32, (lines, 2 * experts), 0)
    c2 = lax.broadcasted_iota(jnp.int32, (lines, 2 * experts), 1)
    goal = (r2 // (4 * pieces) * NX + px) * 2 + r2 // (2 * pieces) % 2
    choose = jnp.where(c2 == goal + r2 // pieces % 2 * experts, 1.0, 0.0).astype(bf16)
    r3 = lax.broadcasted_iota(jnp.int32, (lines, LANES), 0)
    c3 = lax.broadcasted_iota(jnp.int32, (lines, LANES), 1)
    same = (r3 % pieces) == (c3 // seqs)

    def spread(one, two):
        both = jnp.concatenate([one, two], axis=0).astype(bf16)
        wide = jnp.dot(both, copies_of, preferred_element_type=f32).astype(bf16)
        return jnp.where(same, jnp.dot(choose, wide, preferred_element_type=f32), 0.0)

    pick_v[...] = spread(first, second).astype(bf16)

    from_peers(mix_v, mix_send, mix_recv)
    mixed = mix_v[0].astype(f32)
    for i in range(1, NY):
        mixed = mixed + mix_v[i].astype(f32)
    ready(gain_out_v, gain_ffn_v)
    resid = (xf + mixed * rms(mixed) * gain_out_v[...]).astype(bf16)
    rf = resid.astype(f32)
    resid_v[...] = rf
    ffn_in = (rf * rms(rf) * gain_ffn_v[...]).astype(bf16)

    def stacked(array):
        return jnp.concatenate([array[:, k * LANES : (k + 1) * LANES] for k in range(pieces)], axis=0)

    message = jnp.dot(pick_v[...], stacked(ffn_in), preferred_element_type=f32).astype(bf16)
    msg_v[...] = message.reshape(slots, 2 * pieces, LANES)

    def away(slot, src, dst, send_sem, recv_sem):
        return pltpu.make_async_remote_copy(
            src_ref=src, dst_ref=dst, send_sem=send_sem, recv_sem=recv_sem,
            device_id=(partner(slot), y), device_id_type=MESH,
        )

    own = away(self_slot, msg_v.at[self_slot], rows_v.at[y, self_slot], self_send, in_recv.at[self_slot])
    @pl.when(mine)
    def _():
        rows_v[y, self_slot] = msg_v[self_slot]

    def depart(slots_in_turn):
        for slot in slots_in_turn:
            away(slot, msg_v.at[slot], rows_v.at[y, self_slot], out_send, in_recv.at[self_slot]).start()

    @pl.when(z < nz // 2)
    def _():
        depart(around[:-1])

    @pl.when(z >= nz // 2)
    def _():
        depart(around[-2::-1])

    @pl.when(jnp.logical_not(mine))
    def _():
        own.start()

    hi = weight.astype(bf16).astype(f32)
    lo = weight - hi
    pull_hi_v[...] = spread(first * hi, second * hi).T.astype(bf16)
    pull_lo_v[...] = spread(first * lo, second * lo).T.astype(bf16)

    half = 2 * per
    row = lax.broadcasted_iota(jnp.int32, (half * pieces, half * pieces), 0)
    col = lax.broadcasted_iota(jnp.int32, (half * pieces, half * pieces), 1)
    order = jnp.where((row // half == col % pieces) & (row % half == col // pieces), 1.0, 0.0).astype(bf16)
    disorder = jnp.where((col // half == row % pieces) & (col % half == row // pieces), 1.0, 0.0).astype(bf16)

    ready(eg_v, eu_v, ed_v)

    def from_afar(slot, ref, send_sem, recv_sem):
        @pl.when(jnp.logical_not(mine & (self_slot == slot)))
        def _():
            away(slot, ref, ref, send_sem, recv_sem.at[slot]).wait_recv()

    def arrive(g):
        for slot in [g * per + i for i in range(per)]:
            from_afar(slot, rows_v.at[y, slot], out_send, in_recv)
        for step in range(1, NY):
            piece = rows_v.at[y, pl.ds(g * per, per)]
            pltpu.make_async_remote_copy(
                src_ref=piece, dst_ref=piece, send_sem=gat_send, recv_sem=gat_recv.at[step, g],
                device_id=(me, peer(step)), device_id_type=MESH,
            ).start()

    def expert(g):
        for step in range(1, NY):
            source = peer(NY - step)
            piece = rows_v.at[source, pl.ds(g * per, per)]
            pltpu.make_async_remote_copy(
                src_ref=piece, dst_ref=piece, send_sem=gat_send, recv_sem=gat_recv.at[step, g],
                device_id=(me, peer(step)), device_id_type=MESH,
            ).wait_recv()
        side = jnp.concatenate(
            [rows_v[i, pl.ds(g * per, per)].reshape(per * 2 * pieces, LANES) for i in range(NY)], axis=1
        )
        sorted_rows = jnp.dot(order, side, preferred_element_type=f32).astype(bf16)
        inputs = jnp.concatenate(
            [
                jnp.concatenate(
                    [sorted_rows[k * half : (k + 1) * half, i * LANES : (i + 1) * LANES] for k in range(pieces)],
                    axis=1,
                )
                for i in range(NY)
            ],
            axis=0,
        )
        gate = jnp.dot(inputs, eg_v[...], preferred_element_type=f32)
        up = jnp.dot(inputs, eu_v[...], preferred_element_type=f32)
        act = (jax.nn.silu(gate) * up).astype(bf16)
        part = jnp.dot(act, ed_v[...], preferred_element_type=f32).astype(bf16)
        for i in range(NY):
            part_v[g, i] = part[i * half : (i + 1) * half, :]
        for step in range(1, NY):
            pltpu.make_async_remote_copy(
                src_ref=part_v.at[g, peer(step)], dst_ref=red_v.at[g, step], send_sem=red_send,
                recv_sem=red_recv.at[step, g], device_id=(me, peer(step)), device_id_type=MESH,
            ).start()

    def give_back(g):
        total = part_v[g, y].astype(f32)
        for step in range(1, NY):
            pltpu.make_async_remote_copy(
                src_ref=part_v.at[g, peer(step)], dst_ref=red_v.at[g, step], send_sem=red_send,
                recv_sem=red_recv.at[step, g], device_id=(me, peer(step)), device_id_type=MESH,
            ).wait_recv()
        for step in range(1, NY):
            total = total + red_v[g, step].astype(f32)
        lined = jnp.dot(disorder, stacked(total.astype(bf16)), preferred_element_type=f32).astype(bf16)
        back_v[pl.ds(g * per, per)] = lined.reshape(per, 2 * pieces, LANES)
        for slot in [g * per + i for i in range(per)]:
            here = mine & (self_slot == slot)

            @pl.when(jnp.logical_not(here))
            def _():
                away(slot, back_v.at[slot], home_v.at[self_slot], ret_send, ret_recv.at[self_slot]).start()

            @pl.when(here)
            def _():
                home_v[slot] = back_v[slot]

    group = z // (nz // CHUNKS)
    turn = [sum(jnp.where(group == k, order_k[i], 0) for k, order_k in enumerate(TURNS)) for i in range(CHUNKS)]
    for g in turn:
        arrive(g)
    for g in turn:
        expert(g)
    for g in turn:
        give_back(g)

    routed = jnp.zeros((LANES, LANES), f32)
    for g in range(CHUNKS):
        for slot in range(g * per, (g + 1) * per):
            from_afar(slot, home_v.at[slot], ret_send, ret_recv)
        block = home_v[g * per : (g + 1) * per].reshape(per * 2 * pieces, LANES)
        span = slice(g * per * 2 * pieces, (g + 1) * per * 2 * pieces)
        routed = routed + jnp.dot(pull_hi_v[:, span], block, preferred_element_type=f32)
        routed = routed + jnp.dot(pull_lo_v[:, span], block, preferred_element_type=f32)
    flat = jnp.concatenate([routed[k * seqs : (k + 1) * seqs, :] for k in range(pieces)], axis=1)
    last_v[y] = flat.astype(bf16)
    last_copies = to_peers(last_v, last_send, last_recv)
    from_peers(last_v, last_send, last_recv)
    total = last_v[0].astype(f32)
    for i in range(1, NY):
        total = total + last_v[i].astype(f32)
    total_v[...] = total * rms(total)
    ready(gain_last_v)
    quarter = width // NY
    mark = pl.ds(pl.multiple_of(y * quarter, quarter), quarter)
    out_ref[...] = (resid_v[:, mark] + total_v[:, mark] * gain_last_v[...]).astype(bf16)

    for copy in mix_copies + last_copies:
        copy.wait_send()
    rest = msg_v.at[pl.ds(1, slots - 1)]
    away(self_slot, rest, rest, out_send, in_recv.at[0]).wait_send()
    away(self_slot, rest, rest, ret_send, ret_recv.at[0]).wait_send()

    @pl.when(jnp.logical_not(mine))
    def _():
        own.wait_send()
        away(self_slot, msg_v.at[0], msg_v.at[0], ret_send, ret_recv.at[0]).wait_send()

    everything = rows_v.at[pl.ds(0, NY - 1)]
    away(self_slot, everything, everything, gat_send, in_recv.at[0]).wait_send()
    everything = red_v.at[:, pl.ds(1, NY - 1)]
    away(self_slot, everything, everything, red_send, in_recv.at[0]).wait_send()


def per_device(
    nz, tokens, memory, log_scale, mix_gain_in, w_query, w_key, w_value, w_igate, w_fgate, igate_bias, fgate_bias,
    head_gain, w_output, mix_gain_out, ffn_gain_in, routes, route_weights, expert_gate, expert_up, expert_down,
    ffn_gain_out,
):
    f32, bf16 = jnp.float32, jnp.bfloat16
    seqs, width = tokens.shape
    pieces = width // LANES
    key_dim, value_dim = memory.shape[2:]
    slots = 2 * nz
    per = slots // CHUNKS
    lines = slots * 2 * pieces
    hidden = expert_gate.shape[2]
    operands = [
        tokens, memory[:, 0], log_scale.T, mix_gain_in[None], w_query, w_key, w_value, w_igate.T, w_fgate.T,
        igate_bias, fgate_bias, head_gain[None], w_output, mix_gain_out[None], ffn_gain_in[None],
        routes.T, route_weights.T,
        expert_gate[0], expert_up[0], expert_down[0], ffn_gain_out[None],
    ]
    dma, vmem = pltpu.SemaphoreType.DMA, pltpu.VMEM
    scratch = [vmem(a.shape, a.dtype) for a in operands if a.size > 1] + [
        vmem((seqs, value_dim), f32),
        vmem((NY, seqs, width), bf16),
        vmem((lines, LANES), bf16),
        vmem((LANES, lines), bf16),
        vmem((LANES, lines), bf16),
        vmem((slots, 2 * pieces, LANES), bf16),
        vmem((NY, slots, 2 * pieces, LANES), bf16),
        vmem((CHUNKS, NY, 2 * per, width), bf16),
        vmem((CHUNKS, NY, 2 * per, width), bf16),
        vmem((slots, 2 * pieces, LANES), bf16),
        vmem((slots, 2 * pieces, LANES), bf16),
        vmem((NY, seqs, width), bf16),
        vmem((seqs, width), f32),
        vmem((seqs, width), f32),
        dma((len(operands),)), dma((NY,)), dma((NY,)), dma, dma, dma((slots,)), dma, dma((NY, CHUNKS)),
        dma, dma((NY, CHUNKS)), dma, dma((slots,)), dma((NY,)), dma((NY,)),
    ]
    return pl.pallas_call(
        functools.partial(kernel, nz),
        out_shape=vmem((seqs, width // NY), bf16),
        in_specs=[pl.BlockSpec(memory_space=pltpu.HBM if a.size > 1 else pltpu.SMEM) for a in operands],
        out_specs=pl.BlockSpec(memory_space=pltpu.VMEM),
        scratch_shapes=scratch,
        compiler_params=pltpu.CompilerParams(collective_id=0, has_side_effects=True, vmem_limit_bytes=VMEM_LIMIT),
    )(*operands)


def solution(mesh):
    nz = mesh.shape["ep"] // (2 * NX)
    return jax.shard_map(
        functools.partial(per_device, nz),
        mesh=mesh,
        in_specs=(
            P("ep", None), P("ep", "tp", None, None), P("ep", "tp"), P(), P(None, "tp"), P(None, "tp"),
            P(None, "tp"), P(None, "tp"), P(None, "tp"), P("tp"), P("tp"), P("tp"), P("tp", None), P(), P(),
            P("ep", None), P("ep", None), P("ep", None, "tp"), P("ep", None, "tp"), P("ep", "tp", None), P("tp"),
        ),
        out_specs=P("ep", "tp"),
        check_vma=False,
    )
```

```python
import functools

import jax
import jax.numpy as jnp
from jax import lax
from jax.experimental import pallas as pl
from jax.experimental.pallas import tpu as pltpu
from jax.sharding import PartitionSpec as P

EPS = 1e-06
MESH = pl.DeviceIdType.MESH
LANES = 128
NX = 4
NY = 4
CHUNKS = 4
VMEM_LIMIT = 67043328 - 65536
TURNS = ((0, 1, 3, 2), (0, 1, 3, 2), (2, 3, 0, 1), (3, 2, 0, 1))


def rms(values):
    return lax.rsqrt(jnp.mean(values * values, axis=-1, keepdims=True) + EPS)


def kernel(
    nz,
    tokens_h, memory_h, scale_h, gain_in_h, wq_h, wk_h, wv_h, wi_h, wf_h, bi_s, bf_s,
    head_gain_h, wo_h, gain_out_h, gain_ffn_h, routes_h, weights_h, eg_h, eu_h, ed_h, gain_last_h,
    out_ref,
    tokens_v, memory_v, scale_v, gain_in_v, wq_v, wk_v, wv_v, wi_v, wf_v,
    head_gain_v, wo_v, gain_out_v, gain_ffn_v, routes_v, weights_v, eg_v, eu_v, ed_v, gain_last_v,
    recall_v, mix_v, pick_v, pull_hi_v, pull_lo_v, msg_v, rows_v, part_v, red_v, back_v, home_v, last_v, resid_v, total_v,
    load_sem, mix_send, mix_recv, out_send, self_send, in_recv, gat_send, gat_recv,
    red_send, red_recv, ret_send, ret_recv, last_send, last_recv,
):
    f32, bf16 = jnp.float32, jnp.bfloat16
    seqs, width = tokens_v.shape
    pieces = width // LANES
    slots = 2 * nz
    per = slots // CHUNKS
    experts = nz * NX * 2

    me = lax.axis_index("ep")
    y = lax.axis_index("tp")
    c = me % 2
    x = (me // 2) % NX
    z = me // (2 * NX)
    px = (y + NX - x) % NX
    mine = px == x

    self_slot = z * 2 + c

    def partner(slot):
        return (slot // 2 * NX + px) * 2 + slot % 2

    far = sorted(range(nz), key=lambda off: -min(off, nz - off))
    around = [(z + off) % nz * 2 + (1 - c if other else c) for off in far for other in (1, 0)]

    def peer(step):
        return (y + step) % NY

    barrier = pltpu.get_barrier_semaphore()
    for step in range(1, NY):
        pl.semaphore_signal(barrier, inc=1, device_id=(me, peer(step)), device_id_type=MESH)
    for slot in around[:-1]:
        pl.semaphore_signal(barrier, inc=1, device_id=(partner(slot), y), device_id_type=MESH)

    @pl.when(jnp.logical_not(mine))
    def _():
        pl.semaphore_signal(barrier, inc=1, device_id=(partner(self_slot), y), device_id_type=MESH)

    pairs = [
        (routes_h, routes_v), (weights_h, weights_v), (tokens_h, tokens_v), (gain_in_h, gain_in_v),
        (wq_h, wq_v), (wk_h, wk_v), (wv_h, wv_v), (wi_h, wi_v), (wf_h, wf_v),
        (scale_h, scale_v), (memory_h, memory_v), (head_gain_h, head_gain_v), (wo_h, wo_v),
        (gain_out_h, gain_out_v), (gain_ffn_h, gain_ffn_v), (eg_h, eg_v), (eu_h, eu_v), (ed_h, ed_v),
        (gain_last_h, gain_last_v),
    ]
    loads = {}
    for i, (src, dst) in enumerate(pairs):
        loads[id(dst)] = pltpu.make_async_copy(src, dst, load_sem.at[i])
        loads[id(dst)].start()

    def ready(*refs):
        for ref in refs:
            loads[id(ref)].wait()

    ready(tokens_v, gain_in_v)
    xf = tokens_v[...].astype(f32)
    normed = (xf * rms(xf) * gain_in_v[...]).astype(bf16)
    ready(wq_v, wk_v, wv_v)
    key_dim = wq_v.shape[1]
    query = jnp.dot(normed, wq_v[...], preferred_element_type=f32) * key_dim ** (-0.5)
    keys = jnp.dot(normed, wk_v[...], preferred_element_type=f32)
    values = jnp.dot(normed, wv_v[...], preferred_element_type=f32)
    ready(wi_v, wf_v, scale_v)
    nf = normed.astype(f32)
    in_pre = jnp.sum(nf * wi_v[...].astype(f32), axis=-1, keepdims=True) + bi_s[0]
    fg = jnp.sum(nf * wf_v[...].astype(f32), axis=-1, keepdims=True) + bf_s[0]
    forget_log = jnp.minimum(fg, 0.0) - jnp.log1p(jnp.exp(-jnp.abs(fg)))
    tr = lax.broadcasted_iota(jnp.int32, (seqs, seqs), 0)
    tc = lax.broadcasted_iota(jnp.int32, (seqs, seqs), 1)
    log_scale = jnp.sum(
        jnp.where(tr == tc, jnp.broadcast_to(scale_v[...], (seqs, seqs)), 0.0), axis=-1, keepdims=True
    )
    carried = forget_log + log_scale
    new_max = jnp.maximum(carried, in_pre)
    carry_weight = jnp.exp(carried - new_max)
    fresh_weight = jnp.exp(in_pre - new_max)
    match = jnp.sum(query * keys, axis=-1, keepdims=True)
    turned = query.T
    ready(memory_v)
    for s in range(seqs):
        recall_v[s : s + 1, :] = jnp.sum(turned[:, s : s + 1] * memory_v[s], axis=0, keepdims=True)
    read = carry_weight * recall_v[...] + (fresh_weight * match) * values
    ready(head_gain_v, wo_v)
    headout = (read * rms(read) * head_gain_v[...]).astype(bf16)
    mix_v[y] = jnp.dot(headout, wo_v[...], preferred_element_type=f32).astype(bf16)

    pl.semaphore_wait(barrier, NY - 1 + slots - jnp.where(mine, 1, 0))

    def to_peers(ref, send_sem, recv_sem):
        copies = []
        for step in (2, 1, 3):
            copy = pltpu.make_async_remote_copy(
                src_ref=ref.at[y], dst_ref=ref.at[y], send_sem=send_sem.at[step], recv_sem=recv_sem.at[step],
                device_id=(me, peer(step)), device_id_type=MESH,
            )
            copy.start()
            copies.append(copy)
        return copies

    def from_peers(ref, send_sem, recv_sem):
        for step in range(1, NY):
            source = peer(NY - step)
            pltpu.make_async_remote_copy(
                src_ref=ref.at[source], dst_ref=ref.at[source], send_sem=send_sem.at[step],
                recv_sem=recv_sem.at[step], device_id=(me, peer(step)), device_id_type=MESH,
            ).wait_recv()

    mix_copies = to_peers(mix_v, mix_send, mix_recv)

    ready(routes_v, weights_v)
    expert_row = lax.broadcasted_iota(jnp.int32, (experts, seqs), 0)
    named = jnp.zeros((experts, seqs), f32)
    weight = jnp.zeros((experts, seqs), f32)
    for j in range(routes_v.shape[0]):
        hit = expert_row == routes_v[j : j + 1, :]
        named = jnp.where(hit, 1.0, named)
        weight = jnp.where(hit, weights_v[j : j + 1, :], weight)
    row = lax.broadcasted_iota(jnp.int32, (LANES, LANES), 0)
    col = lax.broadcasted_iota(jnp.int32, (LANES, LANES), 1)
    before = jnp.where(row[:seqs, :seqs] < col[:seqs, :seqs], 1.0, 0.0).astype(bf16)
    count = jnp.dot(named.astype(bf16), before, preferred_element_type=f32)
    first = jnp.where(count < 0.5, named, 0.0)
    second = named - first
    copies_of = jnp.where(row[:seqs] == col[:seqs] % seqs, 1.0, 0.0).astype(bf16)
    lines = slots * 2 * pieces
    r2 = lax.broadcasted_iota(jnp.int32, (lines, 2 * experts), 0)
    c2 = lax.broadcasted_iota(jnp.int32, (lines, 2 * experts), 1)
    goal = (r2 // (4 * pieces) * NX + px) * 2 + r2 // (2 * pieces) % 2
    choose = jnp.where(c2 == goal + r2 // pieces % 2 * experts, 1.0, 0.0).astype(bf16)
    r3 = lax.broadcasted_iota(jnp.int32, (lines, LANES), 0)
    c3 = lax.broadcasted_iota(jnp.int32, (lines, LANES), 1)
    same = (r3 % pieces) == (c3 // seqs)

    def spread(one, two):
        both = jnp.concatenate([one, two], axis=0).astype(bf16)
        wide = jnp.dot(both, copies_of, preferred_element_type=f32).astype(bf16)
        return jnp.where(same, jnp.dot(choose, wide, preferred_element_type=f32), 0.0)

    pick_v[...] = spread(first, second).astype(bf16)

    from_peers(mix_v, mix_send, mix_recv)
    mixed = mix_v[0].astype(f32)
    for i in range(1, NY):
        mixed = mixed + mix_v[i].astype(f32)
    ready(gain_out_v, gain_ffn_v)
    resid = (xf + mixed * rms(mixed) * gain_out_v[...]).astype(bf16)
    rf = resid.astype(f32)
    resid_v[...] = rf
    ffn_in = (rf * rms(rf) * gain_ffn_v[...]).astype(bf16)

    def stacked(array):
        return jnp.concatenate([array[:, k * LANES : (k + 1) * LANES] for k in range(pieces)], axis=0)

    message = jnp.dot(pick_v[...], stacked(ffn_in), preferred_element_type=f32).astype(bf16)
    msg_v[...] = message.reshape(slots, 2 * pieces, LANES)

    def away(slot, src, dst, send_sem, recv_sem):
        return pltpu.make_async_remote_copy(
            src_ref=src, dst_ref=dst, send_sem=send_sem, recv_sem=recv_sem,
            device_id=(partner(slot), y), device_id_type=MESH,
        )

    own = away(self_slot, msg_v.at[self_slot], rows_v.at[y, self_slot], self_send, in_recv.at[self_slot])
    @pl.when(mine)
    def _():
        rows_v[y, self_slot] = msg_v[self_slot]

    def depart(slots_in_turn):
        for slot in slots_in_turn:
            away(slot, msg_v.at[slot], rows_v.at[y, self_slot], out_send, in_recv.at[self_slot]).start()

    @pl.when(z < nz // 2)
    def _():
        depart(around[:-1])

    @pl.when(z >= nz // 2)
    def _():
        depart(around[-2::-1])

    @pl.when(jnp.logical_not(mine))
    def _():
        own.start()

    hi = weight.astype(bf16).astype(f32)
    lo = weight - hi
    pull_hi_v[...] = spread(first * hi, second * hi).T.astype(bf16)
    pull_lo_v[...] = spread(first * lo, second * lo).T.astype(bf16)

    half = 2 * per
    row = lax.broadcasted_iota(jnp.int32, (half * pieces, half * pieces), 0)
    col = lax.broadcasted_iota(jnp.int32, (half * pieces, half * pieces), 1)
    order = jnp.where((row // half == col % pieces) & (row % half == col // pieces), 1.0, 0.0).astype(bf16)
    disorder = jnp.where((col // half == row % pieces) & (col % half == row // pieces), 1.0, 0.0).astype(bf16)

    ready(eg_v, eu_v, ed_v)

    def from_afar(slot, ref, send_sem, recv_sem):
        @pl.when(jnp.logical_not(mine & (self_slot == slot)))
        def _():
            away(slot, ref, ref, send_sem, recv_sem.at[slot]).wait_recv()

    def arrive(g):
        for slot in [g * per + i for i in range(per)]:
            from_afar(slot, rows_v.at[y, slot], out_send, in_recv)
        for step in range(1, NY):
            piece = rows_v.at[y, pl.ds(g * per, per)]
            pltpu.make_async_remote_copy(
                src_ref=piece, dst_ref=piece, send_sem=gat_send, recv_sem=gat_recv.at[step, g],
                device_id=(me, peer(step)), device_id_type=MESH,
            ).start()

    def expert(g):
        for step in range(1, NY):
            source = peer(NY - step)
            piece = rows_v.at[source, pl.ds(g * per, per)]
            pltpu.make_async_remote_copy(
                src_ref=piece, dst_ref=piece, send_sem=gat_send, recv_sem=gat_recv.at[step, g],
                device_id=(me, peer(step)), device_id_type=MESH,
            ).wait_recv()
        side = jnp.concatenate(
            [rows_v[i, pl.ds(g * per, per)].reshape(per * 2 * pieces, LANES) for i in range(NY)], axis=1
        )
        sorted_rows = jnp.dot(order, side, preferred_element_type=f32).astype(bf16)
        inputs = jnp.concatenate(
            [
                jnp.concatenate(
                    [sorted_rows[k * half : (k + 1) * half, i * LANES : (i + 1) * LANES] for k in range(pieces)],
                    axis=1,
                )
                for i in range(NY)
            ],
            axis=0,
        )
        gate = jnp.dot(inputs, eg_v[...], preferred_element_type=f32)
        up = jnp.dot(inputs, eu_v[...], preferred_element_type=f32)
        act = (jax.nn.silu(gate) * up).astype(bf16)
        part = jnp.dot(act, ed_v[...], preferred_element_type=f32).astype(bf16)
        for i in range(NY):
            part_v[g, i] = part[i * half : (i + 1) * half, :]
        for step in range(1, NY):
            pltpu.make_async_remote_copy(
                src_ref=part_v.at[g, peer(step)], dst_ref=red_v.at[g, step], send_sem=red_send,
                recv_sem=red_recv.at[step, g], device_id=(me, peer(step)), device_id_type=MESH,
            ).start()

    def give_back(g):
        total = part_v[g, y].astype(f32)
        for step in range(1, NY):
            pltpu.make_async_remote_copy(
                src_ref=part_v.at[g, peer(step)], dst_ref=red_v.at[g, step], send_sem=red_send,
                recv_sem=red_recv.at[step, g], device_id=(me, peer(step)), device_id_type=MESH,
            ).wait_recv()
        for step in range(1, NY):
            total = total + red_v[g, step].astype(f32)
        lined = jnp.dot(disorder, stacked(total.astype(bf16)), preferred_element_type=f32).astype(bf16)
        back_v[pl.ds(g * per, per)] = lined.reshape(per, 2 * pieces, LANES)
        for slot in [g * per + i for i in range(per)]:
            here = mine & (self_slot == slot)

            @pl.when(jnp.logical_not(here))
            def _():
                away(slot, back_v.at[slot], home_v.at[self_slot], ret_send, ret_recv.at[self_slot]).start()

            @pl.when(here)
            def _():
                home_v[slot] = back_v[slot]

    group = z // (nz // CHUNKS)
    turn = [sum(jnp.where(group == k, order_k[i], 0) for k, order_k in enumerate(TURNS)) for i in range(CHUNKS)]
    for g in turn:
        arrive(g)
    for g in turn[:-1]:
        expert(g)
    give_back(turn[0])
    expert(turn[-1])
    for g in turn[1:]:
        give_back(g)

    routed = jnp.zeros((LANES, LANES), f32)
    for g in range(CHUNKS):
        for slot in range(g * per, (g + 1) * per):
            from_afar(slot, home_v.at[slot], ret_send, ret_recv)
        block = home_v[g * per : (g + 1) * per].reshape(per * 2 * pieces, LANES)
        span = slice(g * per * 2 * pieces, (g + 1) * per * 2 * pieces)
        routed = routed + jnp.dot(pull_hi_v[:, span], block, preferred_element_type=f32)
        routed = routed + jnp.dot(pull_lo_v[:, span], block, preferred_element_type=f32)
    flat = jnp.concatenate([routed[k * seqs : (k + 1) * seqs, :] for k in range(pieces)], axis=1)
    last_v[y] = flat.astype(bf16)
    last_copies = to_peers(last_v, last_send, last_recv)
    from_peers(last_v, last_send, last_recv)
    total = last_v[0].astype(f32)
    for i in range(1, NY):
        total = total + last_v[i].astype(f32)
    total_v[...] = total * rms(total)
    ready(gain_last_v)
    quarter = width // NY
    mark = pl.ds(pl.multiple_of(y * quarter, quarter), quarter)
    out_ref[...] = (resid_v[:, mark] + total_v[:, mark] * gain_last_v[...]).astype(bf16)

    for copy in mix_copies + last_copies:
        copy.wait_send()
    rest = msg_v.at[pl.ds(1, slots - 1)]
    away(self_slot, rest, rest, out_send, in_recv.at[0]).wait_send()
    away(self_slot, rest, rest, ret_send, ret_recv.at[0]).wait_send()

    @pl.when(jnp.logical_not(mine))
    def _():
        own.wait_send()
        away(self_slot, msg_v.at[0], msg_v.at[0], ret_send, ret_recv.at[0]).wait_send()

    everything = rows_v.at[pl.ds(0, NY - 1)]
    away(self_slot, everything, everything, gat_send, in_recv.at[0]).wait_send()
    everything = red_v.at[:, pl.ds(1, NY - 1)]
    away(self_slot, everything, everything, red_send, in_recv.at[0]).wait_send()


def per_device(
    nz, tokens, memory, log_scale, mix_gain_in, w_query, w_key, w_value, w_igate, w_fgate, igate_bias, fgate_bias,
    head_gain, w_output, mix_gain_out, ffn_gain_in, routes, route_weights, expert_gate, expert_up, expert_down,
    ffn_gain_out,
):
    f32, bf16 = jnp.float32, jnp.bfloat16
    seqs, width = tokens.shape
    pieces = width // LANES
    key_dim, value_dim = memory.shape[2:]
    slots = 2 * nz
    per = slots // CHUNKS
    lines = slots * 2 * pieces
    hidden = expert_gate.shape[2]
    operands = [
        tokens, memory[:, 0], log_scale.T, mix_gain_in[None], w_query, w_key, w_value, w_igate.T, w_fgate.T,
        igate_bias, fgate_bias, head_gain[None], w_output, mix_gain_out[None], ffn_gain_in[None],
        routes.T, route_weights.T,
        expert_gate[0], expert_up[0], expert_down[0], ffn_gain_out[None],
    ]
    dma, vmem = pltpu.SemaphoreType.DMA, pltpu.VMEM
    scratch = [vmem(a.shape, a.dtype) for a in operands if a.size > 1] + [
        vmem((seqs, value_dim), f32),
        vmem((NY, seqs, width), bf16),
        vmem((lines, LANES), bf16),
        vmem((LANES, lines), bf16),
        vmem((LANES, lines), bf16),
        vmem((slots, 2 * pieces, LANES), bf16),
        vmem((NY, slots, 2 * pieces, LANES), bf16),
        vmem((CHUNKS, NY, 2 * per, width), bf16),
        vmem((CHUNKS, NY, 2 * per, width), bf16),
        vmem((slots, 2 * pieces, LANES), bf16),
        vmem((slots, 2 * pieces, LANES), bf16),
        vmem((NY, seqs, width), bf16),
        vmem((seqs, width), f32),
        vmem((seqs, width), f32),
        dma((len(operands),)), dma((NY,)), dma((NY,)), dma, dma, dma((slots,)), dma, dma((NY, CHUNKS)),
        dma, dma((NY, CHUNKS)), dma, dma((slots,)), dma((NY,)), dma((NY,)),
    ]
    return pl.pallas_call(
        functools.partial(kernel, nz),
        out_shape=vmem((seqs, width // NY), bf16),
        in_specs=[pl.BlockSpec(memory_space=pltpu.HBM if a.size > 1 else pltpu.SMEM) for a in operands],
        out_specs=pl.BlockSpec(memory_space=pltpu.VMEM),
        scratch_shapes=scratch,
        compiler_params=pltpu.CompilerParams(collective_id=0, has_side_effects=True, vmem_limit_bytes=VMEM_LIMIT),
    )(*operands)


def solution(mesh):
    nz = mesh.shape["ep"] // (2 * NX)
    return jax.shard_map(
        functools.partial(per_device, nz),
        mesh=mesh,
        in_specs=(
            P("ep", None), P("ep", "tp", None, None), P("ep", "tp"), P(), P(None, "tp"), P(None, "tp"),
            P(None, "tp"), P(None, "tp"), P(None, "tp"), P("tp"), P("tp"), P("tp"), P("tp", None), P(), P(),
            P("ep", None), P("ep", None), P("ep", None, "tp"), P("ep", None, "tp"), P("ep", "tp", None), P("tp"),
        ),
        out_specs=P("ep", "tp"),
        check_vma=False,
    )
```
